128 devices in a mesh: ep: 64 (over z, y, x), tp: 2 (over core).
Axes of the slice: x: 4, y: 4, z: 4, core: 2. Of those that a mesh axis runs over, the one named last changes fastest.
Arguments:
- hidden: bfloat16 [1408, 2048], P('ep'), may hold values from -6 to 6
- mixer_gain: bfloat16 [2048], replicated, may hold values from 0.099609375 to 1.8984375
- gate_proj: bfloat16 [2048, 1024], P(None, 'tp'), may hold values from -0.125 to 0.125
- value_proj: bfloat16 [2048, 1024], P(None, 'tp'), may hold values from -0.125 to 0.125
- write_proj: bfloat16 [2048, 512], P(None, 'tp'), may hold values from -0.125 to 0.125
- read_proj: bfloat16 [2048, 512], P(None, 'tp'), may hold values from -0.125 to 0.125
- step_proj: bfloat16 [2048, 16], replicated, may hold values from -0.125 to 0.125
- step_bias: float32 [16], replicated, may hold values from -3 to 0
- decay_log: float32 [16], replicated, may hold values from 0 to 2.77
- skip_gain: float32 [16], replicated, may hold values from 0.5 to 2
- value_taps: bfloat16 [4, 1024], replicated, may hold values from -3 to 3
- write_taps: bfloat16 [4, 512], replicated, may hold values from -3 to 3
- read_taps: bfloat16 [4, 512], replicated, may hold values from -3 to 3
- value_tail: bfloat16 [1408, 3, 1024], P('ep', None, 'tp'), may hold values from -6 to 6
- write_tail: bfloat16 [1408, 3, 512], P('ep', None, 'tp'), may hold values from -6 to 6
- read_tail: bfloat16 [1408, 3, 512], P('ep', None, 'tp'), may hold values from -6 to 6
- scan_state: float32 [1408, 16, 64, 128], P('ep', 'tp'), may hold values from -4 to 4
- group_gain: bfloat16 [1024], replicated, may hold values from 0.099609375 to 1.8984375
- out_proj: bfloat16 [1024, 2048], P('tp'), may hold values from -0.1875 to 0.1875
- ffn_gain: bfloat16 [2048], replicated, may hold values from 0.099609375 to 1.8984375
- group_router: bfloat16 [2048, 8], replicated, may hold values from -0.125 to 0.125
- expert_router: bfloat16 [2048, 64], replicated, may hold values from -0.125 to 0.125
- expert_choice: int32 [1408, 3], P('ep'), may hold values from 0 to 63, as said below
- expert_gate: bfloat16 [64, 2048, 1024], P('ep', None, 'tp'), may hold values from -0.125 to 0.125
- expert_up: bfloat16 [64, 2048, 1024], P('ep', None, 'tp'), may hold values from -0.125 to 0.125
- expert_down: bfloat16 [64, 1024, 2048], P('ep', 'tp'), may hold values from -1 to 1
Outputs:
- layer_out: bfloat16 [1408, 2048], P('ep', 'tp')
- new_state: float32 [1408, 16, 64, 128], P('ep', 'tp')
The draws below stay inside these ranges and needn't reach their ends.
Inputs may be any that keep to these rules, and one draw needn't show every extreme that they name: `expert_choice`: every row names 3 different experts of one group (numbers equal in // 8). The 22 rows of one device name no expert more than 3 times, and for every device some expert is named exactly 3 times.
All inputs are finite; a program needn't handle non-finite values.
Results may differ from the reference program's by a relative error of at most 0.017.
Values may be sent and summed in bfloat16 or wider, within the bound.
A program may use at most 128 MiB of HBM per device.

```python
import jax
import jax.numpy as jnp
from jax import lax

D = 2048
HEADS = 16
HEAD_DIM = 64
DI = 1024
BC_GROUPS = 4
STATE_N = 128
TAPS = 4
GROUP_SIZE = 8
TOPK = 3
EXPERT_WIDTH = 1024
SEQ_DEV = 22
TOKENS = 1408
EXPERTS = 64
EXPERT_GROUPS = 8
ROUNDS = 1
CAP = 3
N_EP = 64
N_TP = 2


def draw_expert_choice(key, part):
    level = jax.random.randint(jax.random.fold_in(key, 1), (EXPERTS,), 0, 4)
    order_key = jax.random.fold_in(key, 2)
    orders = jax.vmap(lambda number: jax.random.permutation(jax.random.fold_in(order_key, number), GROUP_SIZE))(jnp.arange(EXPERT_GROUPS))
    remaining = SEQ_DEV - (ROUNDS - 1) * EXPERTS
    block_key = jax.random.fold_in(key, 3)

    def one_block(number):
        own_key = jax.random.fold_in(block_key, number)
        pieces = [jax.random.permutation(jax.random.fold_in(own_key, 10 + turn), EXPERTS) for turn in range(ROUNDS - 1)]
        noise = jax.random.randint(jax.random.fold_in(own_key, 1), (EXPERTS,), 0, 4)
        tiebreak = jax.random.permutation(jax.random.fold_in(own_key, 2), EXPERTS)
        first = jax.random.randint(jax.random.fold_in(own_key, 3), (), 0, EXPERTS)
        spots = jnp.arange(EXPERTS)
        forced = (spots // GROUP_SIZE == first // GROUP_SIZE) & ((spots - first) % GROUP_SIZE < TOPK)
        score = forced.astype(jnp.int32) * (8 * EXPERTS) + (level + noise) * EXPERTS + tiebreak
        picked = lax.top_k(score, remaining)[1]
        slots = jnp.concatenate(pieces + [picked]).astype(jnp.int32)
        shuffle = jax.random.permutation(jax.random.fold_in(own_key, 4), SEQ_DEV)
        return slots[shuffle]
    starts = jax.vmap(one_block)(jnp.arange(TOKENS // SEQ_DEV)).reshape(TOKENS)
    group = starts // GROUP_SIZE
    within = (starts % GROUP_SIZE)[:, None] + jnp.arange(TOPK)[None, :]
    chosen = group[:, None] * GROUP_SIZE + orders[group[:, None], within % GROUP_SIZE]
    return chosen.astype(jnp.int32)


def block_scale(key, extent, cuts, smallest, top_value):
    factor_of = 1.0
    for position, parts in cuts:
        steps = jax.random.uniform(jax.random.fold_in(jax.random.fold_in(key, 6), position), (parts,), jnp.float32, smallest / len(cuts), top_value / len(cuts))
        factor_of = factor_of * jnp.repeat(jnp.exp(steps), extent[position] // parts).reshape((-1,) + (1,) * (len(extent) - 1 - position))
    return factor_of


def bell_draw(key, extent, spread, limit, cuts=(), held_as=jnp.bfloat16):
    array = jax.random.normal(key, extent, jnp.float32) * spread
    if len(cuts) > 0:
        array = block_scale(key, extent, cuts, -0.22, 0.18) * array
    return jnp.clip(array, min=-limit, max=limit).astype(held_as)


def setup_inputs(seed: int = 0) -> dict:
    key_of = jax.random.split(jax.random.key(seed), 27)
    return {
        "hidden": bell_draw(key_of[0], (TOKENS, D), 1.0, 6.0, ((0, 64),)),
        "mixer_gain": jnp.clip(1.0 + 0.18 * jax.random.normal(key_of[1], (D,), jnp.float32), 0.099609375, 1.8984375).astype(jnp.bfloat16),
        "gate_proj": bell_draw(key_of[2], (D, DI), D ** -0.5, 0.125, ((1, 2),)),
        "value_proj": bell_draw(key_of[3], (D, DI), D ** -0.5, 0.125, ((1, 2),)),
        "write_proj": bell_draw(key_of[4], (D, BC_GROUPS * STATE_N), D ** -0.5, 0.125, ((1, 2),)),
        "read_proj": bell_draw(key_of[5], (D, BC_GROUPS * STATE_N), D ** -0.5, 0.125, ((1, 2),)),
        "step_proj": bell_draw(key_of[6], (D, HEADS), D ** -0.5, 0.125),
        "step_bias": jnp.clip(jax.random.uniform(key_of[7], (HEADS,), jnp.float32, -3.0, 0.0), -3.0, 0.0),
        "decay_log": jnp.clip(jax.random.uniform(key_of[8], (HEADS,), jnp.float32, 0.0, 2.77), 0.0, 2.77),
        "skip_gain": jnp.clip(jax.random.uniform(key_of[9], (HEADS,), jnp.float32, 0.5, 2.0), 0.5, 2.0),
        "value_taps": bell_draw(key_of[10], (TAPS, DI), TAPS ** -0.5, 3.0),
        "write_taps": bell_draw(key_of[11], (TAPS, BC_GROUPS * STATE_N), TAPS ** -0.5, 3.0),
        "read_taps": bell_draw(key_of[12], (TAPS, BC_GROUPS * STATE_N), TAPS ** -0.5, 3.0),
        "value_tail": bell_draw(key_of[13], (TOKENS, TAPS - 1, DI), 1.0, 6.0, ((0, 64), (2, 2))),
        "write_tail": bell_draw(key_of[14], (TOKENS, TAPS - 1, BC_GROUPS * STATE_N), 1.0, 6.0, ((0, 64), (2, 2))),
        "read_tail": bell_draw(key_of[15], (TOKENS, TAPS - 1, BC_GROUPS * STATE_N), 1.0, 6.0, ((0, 64), (2, 2))),
        "scan_state": bell_draw(key_of[16], (TOKENS, HEADS, HEAD_DIM, STATE_N), 0.3, 4.0, ((0, 64), (1, 2)), jnp.float32),
        "group_gain": jnp.clip(1.0 + 0.18 * jax.random.normal(key_of[17], (DI,), jnp.float32), 0.099609375, 1.8984375).astype(jnp.bfloat16),
        "out_proj": bell_draw(key_of[18], (DI, D), DI ** -0.5, 0.1875, ((0, 2),)),
        "ffn_gain": jnp.clip(1.0 + 0.18 * jax.random.normal(key_of[19], (D,), jnp.float32), 0.099609375, 1.8984375).astype(jnp.bfloat16),
        "group_router": bell_draw(key_of[20], (D, EXPERT_GROUPS), D ** -0.5, 0.125),
        "expert_router": bell_draw(key_of[21], (D, EXPERTS), D ** -0.5, 0.125),
        "expert_choice": draw_expert_choice(jax.random.fold_in(key_of[26], 71), 0),
        "expert_gate": bell_draw(key_of[23], (EXPERTS, D, EXPERT_WIDTH), D ** -0.5, 0.125, ((0, 64), (2, 2))),
        "expert_up": bell_draw(key_of[24], (EXPERTS, D, EXPERT_WIDTH), D ** -0.5, 0.125, ((0, 64), (2, 2))),
        "expert_down": bell_draw(key_of[25], (EXPERTS, EXPERT_WIDTH, D), (EXPERT_WIDTH // 32) ** -0.5, 1.0, ((0, 64), (1, 2))),
    }


EPSILON = 1e-06

def normed(values, gain):
    widened = values.astype(jnp.float32)
    scale = lax.rsqrt(lax.optimization_barrier(jnp.mean(widened * widened, axis=-1, keepdims=True)) + EPSILON)
    return widened * scale * gain.astype(jnp.float32)

def convolve(history, newest, kernel):
    summed = kernel[-1].astype(jnp.float32) * newest.astype(jnp.float32)
    for offset in range(history.shape[1]):
        summed = summed + kernel[offset].astype(jnp.float32) * history[:, offset].astype(jnp.float32)
    return jax.nn.silu(summed)

def project(left, right):
    return jnp.dot(left, right, preferred_element_type=jnp.float32)

def reference(hidden, mixer_gain, gate_proj, value_proj, write_proj, read_proj, step_proj, step_bias, decay_log, skip_gain, value_taps, write_taps, read_taps, value_tail, write_tail, read_tail, scan_state, group_gain, out_proj, ffn_gain, group_router, expert_router, expert_choice, expert_gate, expert_up, expert_down):
    mixer_in = normed(hidden, mixer_gain).astype(jnp.bfloat16)
    gate_new = project(mixer_in, gate_proj).astype(jnp.bfloat16)
    value_new = project(mixer_in, value_proj).astype(jnp.bfloat16)
    write_new = project(mixer_in, write_proj).astype(jnp.bfloat16)
    read_new = project(mixer_in, read_proj).astype(jnp.bfloat16)
    step_size = jax.nn.softplus(project(mixer_in, step_proj) + step_bias)
    decay = jnp.exp(-step_size * jnp.exp(decay_log))
    value_conv = convolve(value_tail, value_new, value_taps)
    write_conv = convolve(write_tail, write_new, write_taps)
    read_conv = convolve(read_tail, read_new, read_taps)
    per_group = HEADS // BC_GROUPS
    heads_value = value_conv.reshape(TOKENS, HEADS, HEAD_DIM)
    heads_write = jnp.repeat(write_conv.reshape(TOKENS, BC_GROUPS, STATE_N), per_group, axis=1)
    heads_read = jnp.repeat(read_conv.reshape(TOKENS, BC_GROUPS, STATE_N), per_group, axis=1)
    new_state = decay[:, :, None, None] * scan_state + (step_size[:, :, None] * heads_value)[:, :, :, None] * heads_write[:, :, None, :]
    mixed_heads = jnp.einsum('thpn,thn->thp', new_state, heads_read, precision=lax.Precision.HIGHEST) + skip_gain[None, :, None] * heads_value
    gated = mixed_heads.reshape(TOKENS, DI) * jax.nn.silu(gate_new.astype(jnp.float32))
    grouped = gated.reshape(TOKENS, BC_GROUPS, DI // BC_GROUPS)
    grouped = grouped * lax.rsqrt(lax.optimization_barrier(jnp.mean(grouped * grouped, axis=-1, keepdims=True)) + EPSILON)
    mixed = (grouped.reshape(TOKENS, DI) * group_gain.astype(jnp.float32)).astype(jnp.bfloat16)
    residual = hidden.astype(jnp.float32) + project(mixed, out_proj)
    ffn_in = normed(residual, ffn_gain).astype(jnp.bfloat16)
    group_weights = jnp.exp(project(ffn_in, group_router))
    group_prob = group_weights / lax.optimization_barrier(jnp.sum(group_weights, axis=1, keepdims=True))
    group_of = (expert_choice[:, 0] // GROUP_SIZE).astype(jnp.int32)
    chosen_prob = jnp.take_along_axis(group_prob, group_of[:, None], axis=1)
    picked_exp = jnp.exp(jnp.take_along_axis(project(ffn_in, expert_router), expert_choice, axis=1))
    gates = chosen_prob * picked_exp / lax.optimization_barrier(jnp.sum(picked_exp, axis=1, keepdims=True))
    padded = jnp.concatenate([ffn_in, jnp.zeros((1, D), jnp.bfloat16)], axis=0)
    flat_choice = expert_choice.reshape(-1)
    slot_rows = N_EP * CAP
    block = EXPERT_WIDTH // N_TP

    def one_expert(expert):
        hits = jnp.nonzero(flat_choice == expert, size=slot_rows, fill_value=TOKENS * TOPK)[0].astype(jnp.int32)
        sources = jnp.minimum(hits // TOPK, TOKENS).astype(jnp.int32)
        arrived = padded[sources]
        activated = (jax.nn.silu(project(arrived, expert_gate[expert])) * project(arrived, expert_up[expert])).astype(jnp.bfloat16)
        summed = jnp.zeros((slot_rows, D), jnp.float32)
        for shard in range(N_TP):
            partial_value = project(activated[:, shard * block:(shard + 1) * block], expert_down[expert, shard * block:(shard + 1) * block]).astype(jnp.bfloat16)
            summed = summed + lax.optimization_barrier(partial_value).astype(jnp.float32)
        return (hits, summed.astype(jnp.bfloat16))
    hits, outputs = lax.map(one_expert, jnp.arange(EXPERTS, dtype=jnp.int32))
    table = jnp.zeros((TOKENS * TOPK + 1, D), jnp.bfloat16).at[hits.reshape(-1)].set(outputs.reshape(-1, D))
    expert_out = table[:TOKENS * TOPK].reshape(TOKENS, TOPK, D).astype(jnp.float32)
    layer_out = (residual + lax.optimization_barrier(jnp.sum(gates[:, :, None] * expert_out, axis=1))).astype(jnp.bfloat16)
    return (layer_out, new_state)
```

```python
import jax
import jax.numpy as jnp
from jax import lax
from jax.experimental import pallas as pl
from jax.experimental.pallas import tpu as pltpu
from jax.sharding import PartitionSpec as P

GROUP_SIZE = 8


EPSILON = 1e-06


SIDE = 4
PEERS = 64
SLOTS = 3
WIDTH = 2048
HALF = 1024
HIDDEN = 512
TILES = 8
ROWS = SLOTS * TILES
PLANE = 16 * ROWS
TOTAL = PEERS * ROWS
SEQ = 22
PAD = 24
SPREAD = TILES * PAD
BF = jnp.bfloat16
F32 = jnp.float32


def nt_dot(left, right):
    return lax.dot_general(left, right, (((1,), (1,)), ((), ())), preferred_element_type=F32)


def project(left, right):
    return jnp.dot(left, right, preferred_element_type=jnp.float32)


def iota(shape, dim):
    return lax.broadcasted_iota(jnp.int32, shape, dim)


def moe_kernel(
    part_ref,
    hid_ref,
    gain_ref,
    group_ref,
    expert_ref,
    choice_ref,
    gate_hbm,
    up_hbm,
    down_hbm,
    out_ref,
    wg,
    wu,
    wd,
    part_in,
    resid,
    send,
    recv,
    recv_sib,
    comb,
    perm,
    perm_back,
    rows_own,
    rows_sib,
    act,
    y_own,
    y_out,
    y_in,
    back,
    ret,
    w_sem,
    p_send,
    p_recv,
    d_send,
    d_recv,
    f_send,
    f_recv,
    s_send,
    s_recv,
    r_send,
    r_recv,
):
    me = lax.axis_index("ep")
    tp = lax.axis_index("tp")
    mx, my, mz = me % SIDE, (me // SIDE) % SIDE, me // (SIDE * SIDE)

    def ahead(i):
        x = (mx + i % SIDE) % SIDE
        y = (my + (i // SIDE) % SIDE) % SIDE
        z = (mz + i // (SIDE * SIDE)) % SIDE
        return (z * SIDE + y) * SIDE + x

    def behind(i):
        x = (mx + SIDE - i % SIDE) % SIDE
        y = (my + SIDE - (i // SIDE) % SIDE) % SIDE
        z = (mz + SIDE - i // (SIDE * SIDE)) % SIDE
        return (z * SIDE + y) * SIDE + x

    sibling = {"tp": 1 - tp}

    def block(i):
        return pl.ds(pl.multiple_of(i * ROWS, TILES), ROWS)

    bar = pltpu.get_barrier_semaphore()
    pl.semaphore_signal(bar, inc=1, device_id=sibling)

    @pl.loop(1, PEERS)
    def _(i):
        pl.semaphore_signal(bar, inc=1, device_id={"ep": ahead(i)})

    loads = [
        pltpu.make_async_copy(gate_hbm, wg, w_sem.at[0]),
        pltpu.make_async_copy(up_hbm, wu, w_sem.at[1]),
        pltpu.make_async_copy(down_hbm, wd, w_sem.at[2]),
    ]
    for load in loads:
        load.start()

    diagonal = iota((PAD, SEQ), 0) == iota((PAD, SEQ), 1)
    earlier = iota((PAD, SEQ), 1) < iota((PAD, SEQ), 0)
    valid = iota((PAD, 1), 0) < SEQ
    lines = [choice_ref[k : k + 1, :].astype(F32) for k in range(SLOTS)]
    chosen = [jnp.sum(jnp.where(diagonal, line, 0.0), axis=1, keepdims=True) for line in lines]
    codes = []
    for k in range(SLOTS):
        same = jnp.zeros((PAD, SEQ), F32)
        for line in lines:
            same = same + jnp.where((line == chosen[k]) & earlier, 1.0, 0.0)
        rank = jnp.sum(same, axis=1, keepdims=True).astype(jnp.int32)
        number = chosen[k].astype(jnp.int32)
        x = (number % SIDE - mx + SIDE) % SIDE
        y = ((number // SIDE) % SIDE - my + SIDE) % SIDE
        z = (number // (SIDE * SIDE) - mz + SIDE) % SIDE
        slot = ((z * SIDE + y) * SIDE + x) * SLOTS + rank
        codes.append(jnp.where(valid, slot * TILES, -4096))
    lane = iota((PAD, SPREAD), 1)
    on_lane = lane % PAD == iota((PAD, SPREAD), 0)
    tile_of = iota((1, SPREAD), 1) // PAD
    code_rows = [
        jnp.sum(jnp.where(on_lane, code.astype(F32), 0.0), axis=0, keepdims=True).astype(jnp.int32)
        + tile_of
        for code in codes
    ]
    tile_down = iota((SPREAD, 1), 0) // PAD
    code_cols = [jnp.concatenate([code] * TILES, axis=0) + tile_down for code in codes]

    down_ = iota((128, 128), 0)
    over_ = iota((128, 128), 1)
    perm[...] = jnp.where(over_ == (down_ % 16) * TILES + down_ // 16, 1.0, 0.0).astype(BF)
    perm_back[...] = jnp.where(down_ == (over_ % 16) * TILES + over_ // 16, 1.0, 0.0).astype(BF)

    pl.semaphore_wait(bar, PEERS)

    swap = pltpu.make_async_remote_copy(
        part_ref, part_in, p_send, p_recv, device_id=sibling
    )
    swap.start()
    resid[16:PAD, :] = jnp.zeros((PAD - 16, WIDTH), F32)
    swap.wait_recv()
    resid[:SEQ, :] = hid_ref[...].astype(F32) + (part_ref[...] + part_in[...])
    total = resid[...]
    scale = lax.rsqrt(jnp.mean(total * total, axis=1, keepdims=True) + EPSILON)
    ffn_in = (total * scale * gain_ref[...].astype(F32)).astype(BF)

    @pl.when(tp == 0)
    def _():
        rows_own[:PAD, :] = ffn_in[:, :HALF]

    @pl.when(tp == 1)
    def _():
        rows_own[:PAD, :] = ffn_in[:, HALF:]

    mine = rows_own[:PAD, :].astype(F32)
    spread = jnp.concatenate(
        [mine[:, c * 128 : (c + 1) * 128] for c in range(TILES)], axis=0
    ).astype(BF)

    for r in range(SIDE):
        down = iota((PLANE, SPREAD), 0) + r * PLANE
        hit = (down == code_rows[0]) | (down == code_rows[1]) | (down == code_rows[2])
        rows = project(jnp.where(hit, 1.0, 0.0).astype(BF), spread).astype(BF)
        send[r * PLANE : (r + 1) * PLANE, :] = rows
        if r == 0:
            recv[:ROWS, :] = rows[:ROWS, :]

        @pl.loop(1 if r == 0 else 0, 16)
        def _(j):
            i = r * 16 + j
            pltpu.make_async_remote_copy(
                send.at[block(i)],
                recv.at[block(i)],
                d_send,
                d_recv.at[r],
                device_id={"ep": ahead(i)},
            ).start()

    group_exp = jnp.exp(nt_dot(ffn_in, group_ref[...]))
    first = chosen[0].astype(jnp.int32) // GROUP_SIZE
    in_group = iota(group_exp.shape, 1) == first
    chosen_prob = jnp.sum(jnp.where(in_group, group_exp, 0.0), axis=1, keepdims=True) / jnp.sum(
        group_exp, axis=1, keepdims=True
    )
    logits = nt_dot(ffn_in, expert_ref[...])
    place = iota(logits.shape, 1)
    picked = [
        jnp.exp(
            jnp.sum(
                jnp.where(place == number.astype(jnp.int32), logits, 0.0), axis=1, keepdims=True
            )
        )
        for number in chosen
    ]
    below = picked[0] + picked[1] + picked[2]
    gates = [jnp.concatenate([chosen_prob * p / below] * TILES, axis=0) for p in picked]
    for r in range(SIDE):
        over = iota((SPREAD, PLANE), 1) + r * PLANE
        weights = jnp.where(over == code_cols[0], gates[0], 0.0)
        weights = jnp.where(over == code_cols[1], gates[1], weights)
        weights = jnp.where(over == code_cols[2], gates[2], weights)
        comb[:, r * PLANE : (r + 1) * PLANE] = weights.astype(BF)

    def relay(source, target, r):
        for b in range(3 * r, 3 * r + 3):
            moved = project(perm[...], source[b * 128 : (b + 1) * 128, :]).astype(BF)
            for c in range(TILES):
                target[b * 16 : (b + 1) * 16, c * 128 : (c + 1) * 128] = moved[
                    c * 16 : (c + 1) * 16, :
                ]

    def forward(r):
        whole = pl.ds(r * PLANE, PLANE)
        return pltpu.make_async_remote_copy(
            recv.at[whole], recv_sib.at[whole], f_send.at[r], f_recv.at[r], device_id=sibling
        )

    def landed(buffer, sem, r):
        low = ROWS if r == 0 else r * PLANE
        part = buffer.at[pl.ds(low, (r + 1) * PLANE - low)]
        return pltpu.make_async_copy(part, part, sem.at[r])

    for r in range(SIDE):
        landed(recv, d_recv, r).wait()
        forward(r).start()
        relay(recv, rows_own, r)
    for load in loads:
        load.wait()
    for r in range(SIDE):
        forward(r).wait_recv()
        relay(recv_sib, rows_sib, r)

    own_rows = pl.ds(pl.multiple_of(tp * HALF, HALF), HALF)
    sib_rows = pl.ds(pl.multiple_of((1 - tp) * HALF, HALF), HALF)
    for n in range(2):
        cols = slice(n * 256, (n + 1) * 256)
        gated = project(rows_own[...], wg[own_rows, cols]) + project(
            rows_sib[...], wg[sib_rows, cols]
        )
        upped = project(rows_own[...], wu[own_rows, cols]) + project(
            rows_sib[...], wu[sib_rows, cols]
        )
        act[:, cols] = (gated * jax.nn.sigmoid(gated) * upped).astype(BF)

    y_out[...] = project(act[...], wd[:, sib_rows]).astype(BF)
    hand = pltpu.make_async_remote_copy(y_out, y_in, s_send, s_recv, device_id=sibling)
    hand.start()
    y_own[...] = project(act[...], wd[:, own_rows])
    hand.wait_recv()

    for r in range(SIDE):
        for b in range(3 * r, 3 * r + 3):
            lines_ = slice(b * 16, (b + 1) * 16)
            summed = (y_own[lines_, :] + y_in[lines_, :].astype(F32)).astype(BF)
            stacked = jnp.concatenate(
                [summed[:, c * 128 : (c + 1) * 128] for c in range(TILES)], axis=0
            )
            rows = project(perm_back[...], stacked).astype(BF)
            back[b * 128 : (b + 1) * 128, :] = rows
            if b == 0:
                ret[:ROWS, :] = rows[:ROWS, :]

        @pl.loop(1 if r == 0 else 0, 16)
        def _(j):
            i = r * 16 + j
            pltpu.make_async_remote_copy(
                back.at[block(i)],
                ret.at[block(i)],
                r_send,
                r_recv.at[r],
                device_id={"ep": behind(i)},
            ).start()

    merged = None
    for r in range(SIDE):
        landed(ret, r_recv, r).wait()
        cols = slice(r * PLANE, (r + 1) * PLANE)
        term = project(comb[:, cols], ret[cols, :])
        merged = term if merged is None else merged + term
    half = resid[:, own_rows]
    for c in range(TILES):
        cols = slice(c * 128, (c + 1) * 128)
        line = half[:, cols] + merged[c * PAD : (c + 1) * PAD, :]
        out_ref[:, cols] = line[:SEQ, :].astype(BF)

    swap.wait_send()
    hand.wait_send()
    for r in range(SIDE):
        forward(r).wait_send()
    sent = send.at[pl.ds(ROWS, TOTAL - ROWS)]
    pltpu.make_async_copy(sent, sent, d_send).wait()
    gone = back.at[pl.ds(ROWS, TOTAL - ROWS)]
    pltpu.make_async_copy(gone, gone, r_send).wait()


def moe(partial_sum, hidden, gain, group_t, expert_t, choice_t, w_gate, w_up, w_down):
    vmem = pl.BlockSpec(memory_space=pltpu.VMEM)
    anywhere = pl.BlockSpec(memory_space=pl.ANY)
    dma = pltpu.SemaphoreType.DMA
    slots = PEERS * SLOTS
    return pl.pallas_call(
        moe_kernel,
        out_shape=jax.ShapeDtypeStruct((SEQ, HALF), BF),
        in_specs=[vmem] * 6 + [anywhere] * 3,
        out_specs=vmem,
        scratch_shapes=[
            pltpu.VMEM((WIDTH, HIDDEN), BF),
            pltpu.VMEM((WIDTH, HIDDEN), BF),
            pltpu.VMEM((HIDDEN, WIDTH), BF),
            pltpu.VMEM((SEQ, WIDTH), F32),
            pltpu.VMEM((PAD, WIDTH), F32),
            pltpu.VMEM((TOTAL, 128), BF),
            pltpu.VMEM((TOTAL, 128), BF),
            pltpu.VMEM((TOTAL, 128), BF),
            pltpu.VMEM((SPREAD, TOTAL), BF),
            pltpu.VMEM((128, 128), BF),
            pltpu.VMEM((128, 128), BF),
            pltpu.VMEM((slots, HALF), BF),
            pltpu.VMEM((slots, HALF), BF),
            pltpu.VMEM((slots, HIDDEN), BF),
            pltpu.VMEM((slots, HALF), F32),
            pltpu.VMEM((slots, HALF), BF),
            pltpu.VMEM((slots, HALF), BF),
            pltpu.VMEM((TOTAL, 128), BF),
            pltpu.VMEM((TOTAL, 128), BF),
            dma((3,)),
            dma,
            dma,
            dma,
            dma((SIDE,)),
            dma((SIDE,)),
            dma((SIDE,)),
            dma,
            dma,
            dma,
            dma((SIDE,)),
        ],
        compiler_params=pltpu.CompilerParams(
            collective_id=0, has_side_effects=True, vmem_limit_bytes=40 * 1024 * 1024
        ),
        name="moe",
    )(partial_sum, hidden, gain, group_t, expert_t, choice_t, w_gate, w_up, w_down)


def normed(values, gain):
    widened = values.astype(jnp.float32)
    scale = lax.rsqrt(jnp.mean(widened * widened, axis=-1, keepdims=True) + EPSILON)
    return widened * scale * gain.astype(jnp.float32)


def convolve(history, newest, kernel):
    summed = kernel[-1].astype(jnp.float32) * newest.astype(jnp.float32)
    for offset in range(history.shape[1]):
        summed = summed + kernel[offset].astype(jnp.float32) * history[:, offset].astype(
            jnp.float32
        )
    return jax.nn.silu(summed)


def project(left, right):
    return jnp.dot(left, right, preferred_element_type=jnp.float32)


def on_device(
    hidden,
    mixer_gain,
    gate_proj,
    value_proj,
    write_proj,
    read_proj,
    step_proj,
    step_bias,
    decay_log,
    skip_gain,
    value_taps,
    write_taps,
    read_taps,
    value_tail,
    write_tail,
    read_tail,
    scan_state,
    group_gain,
    out_proj,
    ffn_gain,
    group_router,
    expert_router,
    expert_choice,
    expert_gate,
    expert_up,
    expert_down,
):
    tp_count = lax.axis_size("tp")
    ep_count = lax.axis_size("ep")
    tp_index = lax.axis_index("tp")
    seq_rows = hidden.shape[0]
    mixer_in = normed(hidden, mixer_gain).astype(jnp.bfloat16)
    gate_new = project(mixer_in, gate_proj).astype(jnp.bfloat16)
    value_new = project(mixer_in, value_proj).astype(jnp.bfloat16)
    write_new = project(mixer_in, write_proj).astype(jnp.bfloat16)
    read_new = project(mixer_in, read_proj).astype(jnp.bfloat16)
    head_count = step_proj.shape[1] // tp_count
    head_start = tp_index * head_count
    step_local = lax.dynamic_slice_in_dim(step_proj, head_start, head_count, 1)
    bias_local = lax.dynamic_slice_in_dim(step_bias, head_start, head_count, 0)
    rate_local = jnp.exp(lax.dynamic_slice_in_dim(decay_log, head_start, head_count, 0))
    skip_local = lax.dynamic_slice_in_dim(skip_gain, head_start, head_count, 0)
    step_size = jax.nn.softplus(project(mixer_in, step_local) + bias_local)
    decay = jnp.exp(-step_size * rate_local)
    value_width = value_proj.shape[1]
    vector_width = write_proj.shape[1]
    value_conv = convolve(
        value_tail,
        value_new,
        lax.dynamic_slice_in_dim(value_taps, tp_index * value_width, value_width, 1),
    )
    write_conv = convolve(
        write_tail,
        write_new,
        lax.dynamic_slice_in_dim(write_taps, tp_index * vector_width, vector_width, 1),
    )
    read_conv = convolve(
        read_tail,
        read_new,
        lax.dynamic_slice_in_dim(read_taps, tp_index * vector_width, vector_width, 1),
    )
    state_size = scan_state.shape[3]
    group_count = vector_width // state_size
    per_group = head_count // group_count
    heads_value = value_conv.reshape(seq_rows, head_count, value_width // head_count)
    heads_write = jnp.repeat(
        write_conv.reshape(seq_rows, group_count, state_size), per_group, axis=1
    )
    heads_read = jnp.repeat(read_conv.reshape(seq_rows, group_count, state_size), per_group, axis=1)
    new_state = (
        decay[:, :, None, None] * scan_state
        + (step_size[:, :, None] * heads_value)[:, :, :, None] * heads_write[:, :, None, :]
    )
    mixed_heads = (
        jnp.einsum("thpn,thn->thp", new_state, heads_read) + skip_local[None, :, None] * heads_value
    )
    gated = mixed_heads.reshape(seq_rows, value_width) * jax.nn.silu(gate_new.astype(jnp.float32))
    grouped = gated.reshape(seq_rows, group_count, value_width // group_count)
    grouped = grouped * lax.rsqrt(jnp.mean(grouped * grouped, axis=-1, keepdims=True) + EPSILON)
    gain_local = lax.dynamic_slice_in_dim(group_gain, tp_index * value_width, value_width, 0)
    mixed = (grouped.reshape(seq_rows, value_width) * gain_local.astype(jnp.float32)).astype(
        jnp.bfloat16
    )
    layer_out = moe(
        project(mixed, out_proj),
        hidden,
        ffn_gain.reshape(1, -1),
        group_router.T,
        expert_router.T,
        expert_choice.T,
        expert_gate[0],
        expert_up[0],
        expert_down[0],
    )
    return (layer_out, new_state)


def solution(mesh):
    placed = (
        P("ep", None),
        P(),
        P(None, "tp"),
        P(None, "tp"),
        P(None, "tp"),
        P(None, "tp"),
        P(),
        P(),
        P(),
        P(),
        P(),
        P(),
        P(),
        P("ep", None, "tp"),
        P("ep", None, "tp"),
        P("ep", None, "tp"),
        P("ep", "tp", None, None),
        P(),
        P("tp", None),
        P(),
        P(),
        P(),
        P("ep", None),
        P("ep", None, "tp"),
        P("ep", None, "tp"),
        P("ep", "tp", None),
    )
    return jax.shard_map(
        on_device,
        mesh=mesh,
        in_specs=placed,
        out_specs=(P("ep", "tp"), P("ep", "tp", None, None)),
        check_vma=False,
    )
```

```python
import jax
import jax.numpy as jnp
from jax import lax
from jax.experimental import pallas as pl
from jax.experimental.pallas import tpu as pltpu
from jax.sharding import PartitionSpec as P

GROUP_SIZE = 8
EPSILON = 1e-06
SIDE = 4
PEERS = 64
SLOTS = 3
WIDTH = 2048
HALF = 1024
HIDDEN = 512
TILES = 8
ROWS = SLOTS * TILES
PLANE = 16 * ROWS
TOTAL = PEERS * ROWS
SEQ = 22
PAD = 24
SPREAD = TILES * PAD
HEADS = 8
HEAD_DIM = 64
VECTOR = 256
PAIR = 2 * HIDDEN
PAIRS = SEQ // 2
VMEM_ALL = 67043328
BF = jnp.bfloat16
F32 = jnp.float32


def nt_dot(left, right):
    return lax.dot_general(left, right, (((1,), (1,)), ((), ())), preferred_element_type=F32)


def project(left, right):
    return jnp.dot(left, right, preferred_element_type=jnp.float32)


def iota(shape, dim):
    return lax.broadcasted_iota(jnp.int32, shape, dim)


def mix_kernel(*refs):
    sources, (normed_ref, mixed_ref, state_out) = refs[:16], refs[16:19]
    state_hbm, held = sources[-1], refs[19:34]
    state_ref, left, left_t, right, read_t, decays, acc, load_sem, in_sem, out_sem = refs[34:]
    (
        hid_ref,
        gain_ref,
        step_ref,
        bias_ref,
        rate_ref,
        skip_ref,
        value_ref,
        write_ref,
        read_ref,
        value_taps_ref,
        write_taps_ref,
        read_taps_ref,
        value_tail_ref,
        write_tail_ref,
        read_tail_ref,
    ) = held
    tp = lax.axis_index("tp")

    def rows_of(c):
        return pl.ds(pl.multiple_of(c * PAIR, PAIR), PAIR)

    def chunk(c):
        rows = rows_of(c)
        return pltpu.make_async_copy(state_hbm.at[rows], state_ref.at[rows], in_sem.at[c])

    def chunk_out(c):
        rows = rows_of(c)
        return pltpu.make_async_copy(state_ref.at[rows], state_out.at[rows], out_sem.at[c])

    loads = [
        pltpu.make_async_copy(sources[n], held[n], load_sem.at[n]) for n in range(len(held))
    ]
    for load in loads:
        load.start()
    for c in range(PAIRS):
        chunk(c).start()
    for load in loads[:6]:
        load.wait()

    wide = hid_ref[...].astype(F32)
    scale = lax.rsqrt(jnp.mean(wide * wide, axis=1, keepdims=True) + EPSILON)
    mixer_in = (wide * scale * gain_ref[...].astype(F32).reshape(1, WIDTH)).astype(BF)
    normed_ref[...] = mixer_in

    def local_heads(line):
        return jnp.where(tp == 0, line[:, :HEADS], line[:, HEADS:])

    bias = local_heads(bias_ref[...])
    rate = jnp.exp(local_heads(rate_ref[...]))
    skip = local_heads(skip_ref[...])
    raw = local_heads(nt_dot(mixer_in, step_ref[...])) + bias
    step = jnp.maximum(raw, 0.0) + jnp.log1p(jnp.exp(-jnp.abs(raw)))
    decay = jnp.exp(-step * rate)
    for h in range(HEADS):
        decays[:SEQ, h, :] = jnp.broadcast_to(decay[:, h : h + 1], (SEQ, 128))

    def convolve(tail_ref, newest, taps_ref, width):
        cols = pl.ds(pl.multiple_of(tp * width, width), width)
        taps = taps_ref[:, cols].astype(F32)
        summed = taps[3:4, :] * newest.astype(BF).astype(F32)
        for offset in range(3):
            summed = summed + taps[offset : offset + 1, :] * tail_ref[offset].astype(F32)
        return summed * jax.nn.sigmoid(summed)

    for load in loads[6:]:
        load.wait()
    value = convolve(value_tail_ref, project(mixer_in, value_ref[...]), value_taps_ref, HIDDEN)
    write = convolve(write_tail_ref, project(mixer_in, write_ref[...]), write_taps_ref, VECTOR)
    read = convolve(read_tail_ref, project(mixer_in, read_ref[...]), read_taps_ref, VECTOR)

    head_of = iota((1, HIDDEN), 1) // HEAD_DIM
    step_wide = jnp.zeros((SEQ, HIDDEN), F32)
    skip_wide = jnp.zeros((1, HIDDEN), F32)
    for h in range(HEADS):
        step_wide = jnp.where(head_of == h, step[:, h : h + 1], step_wide)
        skip_wide = jnp.where(head_of == h, skip[:, h : h + 1], skip_wide)
    drive = step_wide * value

    drive_high = drive.astype(BF).astype(F32)
    write_high = write.astype(BF).astype(F32)
    left[...] = jnp.zeros((128, HIDDEN), F32)
    left[:SEQ, :] = drive_high
    left[32 : 32 + SEQ, :] = drive_high
    left[64 : 64 + SEQ, :] = drive - drive_high
    right[...] = jnp.zeros((128, VECTOR), F32)
    right[:SEQ, :] = write_high
    right[32 : 32 + SEQ, :] = write - write_high
    right[64 : 64 + SEQ, :] = write_high
    for b in range(HIDDEN // 128):
        part = slice(b * 128, (b + 1) * 128)
        left_t[part, :] = left[:, part].T.astype(BF)
    left[:, :VECTOR] = jnp.zeros((128, VECTOR), F32)
    left[:SEQ, :VECTOR] = read
    for g in range(2):
        part = slice(g * 128, (g + 1) * 128)
        read_t[part, :] = left[:, part].T
    acc[...] = jnp.zeros((HIDDEN, 128), F32)

    stacked_row = iota((128, 128), 0) % 32
    lane = iota((128, 128), 1)

    @pl.loop(0, PAIRS)
    def _(c):
        chunk(c).wait()
        for g in range(2):
            part = slice(g * 128, (g + 1) * 128)
            pair = [2 * c, 2 * c + 1]
            outer = project(
                left_t[g * 256 : (g + 1) * 256, :],
                jnp.concatenate(
                    [jnp.where(stacked_row == t, right[:, part], 0.0) for t in pair], axis=1
                ).astype(BF),
            )
            fresh = []
            for k in range(2):
                pieces = []
                for h in range(4):
                    rows = pl.ds(
                        pl.multiple_of(c * PAIR + k * HIDDEN + g * 256 + h * HEAD_DIM, HEAD_DIM),
                        HEAD_DIM,
                    )
                    keep = decays[2 * c + k, g * 4 + h : g * 4 + h + 1, :]
                    new = (
                        keep * state_ref[rows, :]
                        + outer[h * HEAD_DIM : (h + 1) * HEAD_DIM, k * 128 : (k + 1) * 128]
                    )
                    state_ref[rows, :] = new
                    pieces.append(new.astype(BF))
                fresh.append(jnp.concatenate(pieces, axis=0))
            reader = jnp.concatenate(
                [jnp.where(lane == t, read_t[part, :], 0.0) for t in pair], axis=0
            ).astype(BF)
            acc[g * 256 : (g + 1) * 256, :] += project(jnp.concatenate(fresh, axis=1), reader)
        chunk_out(c).start()

    for b in range(HIDDEN // 128):
        part = slice(b * 128, (b + 1) * 128)
        mixed_ref[:, part] = acc[part, :].T[:SEQ, :] + skip_wide[:, part] * value[:, part]

    for c in range(PAIRS):
        chunk_out(c).wait()


def mix(*operands):
    vmem = pl.BlockSpec(memory_space=pltpu.VMEM)
    hbm = pl.BlockSpec(memory_space=pltpu.HBM)
    dma = pltpu.SemaphoreType.DMA
    return pl.pallas_call(
        mix_kernel,
        out_shape=(
            jax.ShapeDtypeStruct((SEQ, WIDTH), BF),
            jax.ShapeDtypeStruct((SEQ, HIDDEN), F32),
            jax.ShapeDtypeStruct((SEQ * HIDDEN, 128), F32),
        ),
        in_specs=[hbm] * len(operands),
        out_specs=(vmem, vmem, hbm),
        scratch_shapes=[pltpu.VMEM(x.shape, x.dtype) for x in operands]
        + [
            pltpu.VMEM((128, HIDDEN), F32),
            pltpu.VMEM((HIDDEN, 128), BF),
            pltpu.VMEM((128, VECTOR), F32),
            pltpu.VMEM((VECTOR, 128), F32),
            pltpu.VMEM((PAD, HEADS, 128), F32),
            pltpu.VMEM((HIDDEN, 128), F32),
            dma((len(operands) - 1,)),
            dma((PAIRS,)),
            dma((PAIRS,)),
        ],
        compiler_params=pltpu.CompilerParams(vmem_limit_bytes=VMEM_ALL),
        name="mix",
    )(*operands)


def moe_kernel(*refs):
    sources, out_ref, held = refs[:13], refs[13], refs[14:27]
    (
        normed_ref,
        gate_proj,
        heads_ref,
        group_gain_ref,
        out_proj,
        hid_ref,
        gain_ref,
        group_ref,
        expert_ref,
        choice_ref,
        wg,
        wu,
        wd,
    ) = held
    (
        part_ref,
        part_in,
        resid,
        send,
        recv,
        recv_sib,
        comb,
        perm,
        perm_back,
        rows_own,
        rows_sib,
        act,
        y_own,
        y_out,
        y_in,
        back,
        ret,
        w_sem,
        p_send,
        p_recv,
        d_send,
        d_recv,
        f_send,
        f_recv,
        s_send,
        s_recv,
        r_send,
        r_recv,
    ) = refs[27:]
    me = lax.axis_index("ep")
    tp = lax.axis_index("tp")
    mx, my, mz = me % SIDE, (me // SIDE) % SIDE, me // (SIDE * SIDE)

    def ahead(i):
        x = (mx + i % SIDE) % SIDE
        y = (my + (i // SIDE) % SIDE) % SIDE
        z = (mz + i // (SIDE * SIDE)) % SIDE
        return (z * SIDE + y) * SIDE + x

    def behind(i):
        x = (mx + SIDE - i % SIDE) % SIDE
        y = (my + SIDE - (i // SIDE) % SIDE) % SIDE
        z = (mz + SIDE - i // (SIDE * SIDE)) % SIDE
        return (z * SIDE + y) * SIDE + x

    sibling = {"tp": 1 - tp}

    def block(i):
        return pl.ds(pl.multiple_of(i * ROWS, TILES), ROWS)

    loads = [
        pltpu.make_async_copy(sources[n], held[n], w_sem.at[n]) for n in range(len(held))
    ]
    for n in [9, 0, 1, 2, 3, 4, 5, 6, 7, 8, 10, 11, 12]:
        loads[n].start()

    bar = pltpu.get_barrier_semaphore()
    pl.semaphore_signal(bar, inc=1, device_id=sibling)

    @pl.loop(1, PEERS)
    def _(i):
        pl.semaphore_signal(bar, inc=1, device_id={"ep": ahead(i)})

    loads[9].wait()
    diagonal = iota((PAD, SEQ), 0) == iota((PAD, SEQ), 1)
    earlier = iota((PAD, SEQ), 1) < iota((PAD, SEQ), 0)
    valid = iota((PAD, 1), 0) < SEQ
    lines = [choice_ref[k : k + 1, :].astype(F32) for k in range(SLOTS)]
    chosen = [jnp.sum(jnp.where(diagonal, line, 0.0), axis=1, keepdims=True) for line in lines]
    codes = []
    for k in range(SLOTS):
        same = jnp.zeros((PAD, SEQ), F32)
        for line in lines:
            same = same + jnp.where((line == chosen[k]) & earlier, 1.0, 0.0)
        rank = jnp.sum(same, axis=1, keepdims=True).astype(jnp.int32)
        number = chosen[k].astype(jnp.int32)
        x = (number % SIDE - mx + SIDE) % SIDE
        y = ((number // SIDE) % SIDE - my + SIDE) % SIDE
        z = (number // (SIDE * SIDE) - mz + SIDE) % SIDE
        slot = ((z * SIDE + y) * SIDE + x) * SLOTS + rank
        codes.append(jnp.where(valid, slot * TILES, -4096))
    lane = iota((PAD, SPREAD), 1)
    on_lane = lane % PAD == iota((PAD, SPREAD), 0)
    tile_of = iota((1, SPREAD), 1) // PAD
    code_rows = [
        jnp.sum(jnp.where(on_lane, code.astype(F32), 0.0), axis=0, keepdims=True).astype(jnp.int32)
        + tile_of
        for code in codes
    ]
    tile_down = iota((SPREAD, 1), 0) // PAD
    code_cols = [jnp.concatenate([code] * TILES, axis=0) + tile_down for code in codes]

    down_ = iota((128, 128), 0)
    over_ = iota((128, 128), 1)
    perm[...] = jnp.where(over_ == (down_ % 16) * TILES + down_ // 16, 1.0, 0.0).astype(BF)
    perm_back[...] = jnp.where(down_ == (over_ % 16) * TILES + over_ // 16, 1.0, 0.0).astype(BF)

    for load in loads[:4]:
        load.wait()
    gate = project(normed_ref[...], gate_proj[...]).astype(BF).astype(F32)
    gated = heads_ref[...] * (gate * jax.nn.sigmoid(gate))
    mixer_cols = pl.ds(pl.multiple_of(tp * HIDDEN, HIDDEN), HIDDEN)
    group_gain = group_gain_ref[mixer_cols].astype(F32).reshape(1, HIDDEN)
    mixed = []
    for g in range(2):
        cols = slice(g * 256, (g + 1) * 256)
        part = gated[:, cols]
        spread_ = lax.rsqrt(jnp.mean(part * part, axis=1, keepdims=True) + EPSILON)
        mixed.append(part * spread_ * group_gain[:, cols])
    mixed = jnp.concatenate(mixed, axis=1).astype(BF)
    loads[4].wait()
    part_ref[...] = project(mixed, out_proj[...])

    pl.semaphore_wait(bar, PEERS)

    swap = pltpu.make_async_remote_copy(
        part_ref, part_in, p_send, p_recv, device_id=sibling
    )
    swap.start()
    for load in loads[5:9]:
        load.wait()
    resid[16:PAD, :] = jnp.zeros((PAD - 16, WIDTH), F32)
    swap.wait_recv()
    resid[:SEQ, :] = hid_ref[...].astype(F32) + (part_ref[...] + part_in[...])
    total = resid[...]
    scale = lax.rsqrt(jnp.mean(total * total, axis=1, keepdims=True) + EPSILON)
    ffn_in = (total * scale * gain_ref[...].astype(F32).reshape(1, WIDTH)).astype(BF)

    @pl.when(tp == 0)
    def _():
        rows_own[:PAD, :] = ffn_in[:, :HALF]

    @pl.when(tp == 1)
    def _():
        rows_own[:PAD, :] = ffn_in[:, HALF:]

    mine = rows_own[:PAD, :].astype(F32)
    spread = jnp.concatenate(
        [mine[:, c * 128 : (c + 1) * 128] for c in range(TILES)], axis=0
    ).astype(BF)

    for r in range(SIDE):
        down = iota((PLANE, SPREAD), 0) + r * PLANE
        hit = (down == code_rows[0]) | (down == code_rows[1]) | (down == code_rows[2])
        rows = project(jnp.where(hit, 1.0, 0.0).astype(BF), spread).astype(BF)
        send[r * PLANE : (r + 1) * PLANE, :] = rows
        if r == 0:
            recv[:ROWS, :] = rows[:ROWS, :]

        @pl.loop(1 if r == 0 else 0, 16)
        def _(j):
            i = r * 16 + j
            pltpu.make_async_remote_copy(
                send.at[block(i)],
                recv.at[block(i)],
                d_send,
                d_recv.at[r],
                device_id={"ep": ahead(i)},
            ).start()

    group_exp = jnp.exp(nt_dot(ffn_in, group_ref[...]))
    first = chosen[0].astype(jnp.int32) // GROUP_SIZE
    in_group = iota(group_exp.shape, 1) == first
    chosen_prob = jnp.sum(jnp.where(in_group, group_exp, 0.0), axis=1, keepdims=True) / jnp.sum(
        group_exp, axis=1, keepdims=True
    )
    logits = nt_dot(ffn_in, expert_ref[...])
    place = iota(logits.shape, 1)
    picked = [
        jnp.exp(
            jnp.sum(
                jnp.where(place == number.astype(jnp.int32), logits, 0.0), axis=1, keepdims=True
            )
        )
        for number in chosen
    ]
    below = picked[0] + picked[1] + picked[2]
    gates = [jnp.concatenate([chosen_prob * p / below] * TILES, axis=0) for p in picked]
    for r in range(SIDE):
        over = iota((SPREAD, PLANE), 1) + r * PLANE
        weights = jnp.where(over == code_cols[0], gates[0], 0.0)
        weights = jnp.where(over == code_cols[1], gates[1], weights)
        weights = jnp.where(over == code_cols[2], gates[2], weights)
        comb[:, r * PLANE : (r + 1) * PLANE] = weights.astype(BF)

    def relay(source, target, r):
        for b in range(3 * r, 3 * r + 3):
            moved = project(perm[...], source[b * 128 : (b + 1) * 128, :]).astype(BF)
            for c in range(TILES):
                target[b * 16 : (b + 1) * 16, c * 128 : (c + 1) * 128] = moved[
                    c * 16 : (c + 1) * 16, :
                ]

    def forward(r):
        whole = pl.ds(r * PLANE, PLANE)
        return pltpu.make_async_remote_copy(
            recv.at[whole], recv_sib.at[whole], f_send.at[r], f_recv.at[r], device_id=sibling
        )

    def landed(buffer, sem, r):
        low = ROWS if r == 0 else r * PLANE
        part = buffer.at[pl.ds(low, (r + 1) * PLANE - low)]
        return pltpu.make_async_copy(part, part, sem.at[r])

    for r in range(SIDE):
        landed(recv, d_recv, r).wait()
        forward(r).start()
        relay(recv, rows_own, r)
    for load in loads[10:]:
        load.wait()
    for r in range(SIDE):
        forward(r).wait_recv()
        relay(recv_sib, rows_sib, r)

    own_rows = pl.ds(pl.multiple_of(tp * HALF, HALF), HALF)
    sib_rows = pl.ds(pl.multiple_of((1 - tp) * HALF, HALF), HALF)
    for n in range(2):
        cols = slice(n * 256, (n + 1) * 256)
        gated = project(rows_own[...], wg[own_rows, cols]) + project(
            rows_sib[...], wg[sib_rows, cols]
        )
        upped = project(rows_own[...], wu[own_rows, cols]) + project(
            rows_sib[...], wu[sib_rows, cols]
        )
        act[:, cols] = (gated * jax.nn.sigmoid(gated) * upped).astype(BF)

    y_out[...] = project(act[...], wd[:, sib_rows]).astype(BF)
    hand = pltpu.make_async_remote_copy(y_out, y_in, s_send, s_recv, device_id=sibling)
    hand.start()
    y_own[...] = project(act[...], wd[:, own_rows])
    hand.wait_recv()

    for r in range(SIDE):
        for b in range(3 * r, 3 * r + 3):
            lines_ = slice(b * 16, (b + 1) * 16)
            summed = (y_own[lines_, :] + y_in[lines_, :].astype(F32)).astype(BF)
            stacked = jnp.concatenate(
                [summed[:, c * 128 : (c + 1) * 128] for c in range(TILES)], axis=0
            )
            rows = project(perm_back[...], stacked).astype(BF)
            back[b * 128 : (b + 1) * 128, :] = rows
            if b == 0:
                ret[:ROWS, :] = rows[:ROWS, :]

        @pl.loop(1 if r == 0 else 0, 16)
        def _(j):
            i = r * 16 + j
            pltpu.make_async_remote_copy(
                back.at[block(i)],
                ret.at[block(i)],
                r_send,
                r_recv.at[r],
                device_id={"ep": behind(i)},
            ).start()

    merged = None
    for r in range(SIDE):
        landed(ret, r_recv, r).wait()
        cols = slice(r * PLANE, (r + 1) * PLANE)
        term = project(comb[:, cols], ret[cols, :])
        merged = term if merged is None else merged + term
    half = resid[:, own_rows]
    for c in range(TILES):
        cols = slice(c * 128, (c + 1) * 128)
        line = half[:, cols] + merged[c * PAD : (c + 1) * PAD, :]
        out_ref[:, cols] = line[:SEQ, :].astype(BF)

    swap.wait_send()
    hand.wait_send()
    for r in range(SIDE):
        forward(r).wait_send()
    sent = send.at[pl.ds(ROWS, TOTAL - ROWS)]
    pltpu.make_async_copy(sent, sent, d_send).wait()
    gone = back.at[pl.ds(ROWS, TOTAL - ROWS)]
    pltpu.make_async_copy(gone, gone, r_send).wait()


def moe(*operands):
    vmem = pl.BlockSpec(memory_space=pltpu.VMEM)
    hbm = pl.BlockSpec(memory_space=pltpu.HBM)
    dma = pltpu.SemaphoreType.DMA
    slots = PEERS * SLOTS
    return pl.pallas_call(
        moe_kernel,
        out_shape=jax.ShapeDtypeStruct((SEQ, HALF), BF),
        in_specs=[hbm] * len(operands),
        out_specs=vmem,
        scratch_shapes=[pltpu.VMEM(x.shape, x.dtype) for x in operands]
        + [
            pltpu.VMEM((SEQ, WIDTH), F32),
            pltpu.VMEM((SEQ, WIDTH), F32),
            pltpu.VMEM((PAD, WIDTH), F32),
            pltpu.VMEM((TOTAL, 128), BF),
            pltpu.VMEM((TOTAL, 128), BF),
            pltpu.VMEM((TOTAL, 128), BF),
            pltpu.VMEM((SPREAD, TOTAL), BF),
            pltpu.VMEM((128, 128), BF),
            pltpu.VMEM((128, 128), BF),
            pltpu.VMEM((slots, HALF), BF),
            pltpu.VMEM((slots, HALF), BF),
            pltpu.VMEM((slots, HIDDEN), BF),
            pltpu.VMEM((slots, HALF), F32),
            pltpu.VMEM((slots, HALF), BF),
            pltpu.VMEM((slots, HALF), BF),
            pltpu.VMEM((TOTAL, 128), BF),
            pltpu.VMEM((TOTAL, 128), BF),
            dma((len(operands),)),
            dma,
            dma,
            dma,
            dma((SIDE,)),
            dma((SIDE,)),
            dma((SIDE,)),
            dma,
            dma,
            dma,
            dma((SIDE,)),
        ],
        compiler_params=pltpu.CompilerParams(
            collective_id=0, has_side_effects=True, vmem_limit_bytes=VMEM_ALL
        ),
        name="moe",
    )(*operands)


def on_device(
    hidden,
    mixer_gain,
    gate_proj,
    value_proj,
    write_proj,
    read_proj,
    step_proj,
    step_bias,
    decay_log,
    skip_gain,
    value_taps,
    write_taps,
    read_taps,
    value_tail,
    write_tail,
    read_tail,
    scan_state,
    group_gain,
    out_proj,
    ffn_gain,
    group_router,
    expert_router,
    expert_choice,
    expert_gate,
    expert_up,
    expert_down,
):
    mixer_in, heads, new_state = mix(
        hidden,
        mixer_gain,
        step_proj.T,
        step_bias.reshape(1, -1),
        decay_log.reshape(1, -1),
        skip_gain.reshape(1, -1),
        value_proj,
        write_proj,
        read_proj,
        value_taps,
        write_taps,
        read_taps,
        value_tail.transpose(1, 0, 2),
        write_tail.transpose(1, 0, 2),
        read_tail.transpose(1, 0, 2),
        scan_state.reshape(SEQ * HIDDEN, 128),
    )
    layer_out = moe(
        mixer_in,
        gate_proj,
        heads,
        group_gain,
        out_proj,
        hidden,
        ffn_gain,
        group_router.T,
        expert_router.T,
        expert_choice.T,
        expert_gate[0],
        expert_up[0],
        expert_down[0],
    )
    return (layer_out, new_state.reshape(scan_state.shape))


def solution(mesh):
    placed = (
        P("ep", None),
        P(),
        P(None, "tp"),
        P(None, "tp"),
        P(None, "tp"),
        P(None, "tp"),
        P(),
        P(),
        P(),
        P(),
        P(),
        P(),
        P(),
        P("ep", None, "tp"),
        P("ep", None, "tp"),
        P("ep", None, "tp"),
        P("ep", "tp", None, None),
        P(),
        P("tp", None),
        P(),
        P(),
        P(),
        P("ep", None),
        P("ep", None, "tp"),
        P("ep", None, "tp"),
        P("ep", "tp", None),
    )
    return jax.shard_map(
        on_device,
        mesh=mesh,
        in_specs=placed,
        out_specs=(P("ep", "tp"), P("ep", "tp", None, None)),
        check_vma=False,
    )
```

```python
import jax
import jax.numpy as jnp
from jax import lax
from jax.experimental import pallas as pl
from jax.experimental.pallas import tpu as pltpu
from jax.sharding import PartitionSpec as P

GROUP_SIZE = 8
EPSILON = 1e-06
SIDE = 4
PEERS = 64
ORDER = (2, 3, 1, 0)
BATCH = 96
SLOTS = 3
WIDTH = 2048
HALF = 1024
HIDDEN = 512
TILES = 8
ROWS = SLOTS * TILES
PLANE = 16 * ROWS
TOTAL = PEERS * ROWS
SEQ = 22
PAD = 24
SPREAD = TILES * PAD
HEADS = 8
HEAD_DIM = 64
VECTOR = 256
PAIR = 2 * HIDDEN
PAIRS = SEQ // 2
VMEM_ALL = 67043328
BF = jnp.bfloat16
F32 = jnp.float32


def nt_dot(left, right):
    return lax.dot_general(left, right, (((1,), (1,)), ((), ())), preferred_element_type=F32)


def project(left, right):
    return jnp.dot(left, right, preferred_element_type=jnp.float32)


def iota(shape, dim):
    return lax.broadcasted_iota(jnp.int32, shape, dim)


def mix_kernel(*refs):
    sources, (normed_ref, mixed_ref, state_out) = refs[:16], refs[16:19]
    state_hbm, held = sources[-1], refs[19:34]
    state_ref, left, left_t, right, read_t, decays, acc, load_sem, in_sem, out_sem = refs[34:]
    (
        hid_ref,
        gain_ref,
        step_ref,
        bias_ref,
        rate_ref,
        skip_ref,
        value_ref,
        write_ref,
        read_ref,
        value_taps_ref,
        write_taps_ref,
        read_taps_ref,
        value_tail_ref,
        write_tail_ref,
        read_tail_ref,
    ) = held
    tp = lax.axis_index("tp")

    def rows_of(c):
        return pl.ds(c * PAIR, PAIR)

    def chunk(c):
        rows = rows_of(c)
        return pltpu.make_async_copy(state_hbm.at[rows], state_ref.at[rows], in_sem.at[c])

    def chunk_out(c):
        rows = rows_of(c)
        return pltpu.make_async_copy(state_ref.at[rows], state_out.at[rows], out_sem.at[c])

    loads = [
        pltpu.make_async_copy(sources[n], held[n], load_sem.at[n]) for n in range(len(held))
    ]
    for load in loads:
        load.start()
    for load in loads[:6]:
        load.wait()

    wide = hid_ref[...].astype(F32)
    scale = lax.rsqrt(jnp.mean(wide * wide, axis=1, keepdims=True) + EPSILON)
    mixer_in = (wide * scale * gain_ref[...].astype(F32).reshape(1, WIDTH)).astype(BF)
    normed_ref[...] = mixer_in

    def local_heads(line):
        return jnp.where(tp == 0, line[:, :HEADS], line[:, HEADS:])

    bias = local_heads(bias_ref[...])
    rate = jnp.exp(local_heads(rate_ref[...]))
    skip = local_heads(skip_ref[...])
    raw = local_heads(nt_dot(mixer_in, step_ref[...])) + bias
    step = jnp.maximum(raw, 0.0) + jnp.log1p(jnp.exp(-jnp.abs(raw)))
    decay = jnp.exp(-step * rate)
    for h in range(HEADS):
        decays[:SEQ, h, :] = jnp.broadcast_to(decay[:, h : h + 1], (SEQ, 128))

    def convolve(tail_ref, newest, taps_ref, width):
        cols = pl.ds(pl.multiple_of(tp * width, width), width)
        taps = taps_ref[:, cols].astype(F32)
        summed = taps[3:4, :] * newest.astype(BF).astype(F32)
        for offset in range(3):
            summed = summed + taps[offset : offset + 1, :] * tail_ref[offset].astype(F32)
        return summed * jax.nn.sigmoid(summed)

    for c in range(PAIRS):
        chunk(c).start()
    for load in loads[6:]:
        load.wait()
    value = convolve(value_tail_ref, project(mixer_in, value_ref[...]), value_taps_ref, HIDDEN)
    write = convolve(write_tail_ref, project(mixer_in, write_ref[...]), write_taps_ref, VECTOR)
    read = convolve(read_tail_ref, project(mixer_in, read_ref[...]), read_taps_ref, VECTOR)

    head_of = iota((1, HIDDEN), 1) // HEAD_DIM
    step_wide = jnp.zeros((SEQ, HIDDEN), F32)
    skip_wide = jnp.zeros((1, HIDDEN), F32)
    for h in range(HEADS):
        step_wide = jnp.where(head_of == h, step[:, h : h + 1], step_wide)
        skip_wide = jnp.where(head_of == h, skip[:, h : h + 1], skip_wide)
    drive = step_wide * value

    drive_high = drive.astype(BF).astype(F32)
    write_high = write.astype(BF).astype(F32)
    left[...] = jnp.zeros((128, HIDDEN), F32)
    left[:SEQ, :] = drive_high
    left[32 : 32 + SEQ, :] = drive_high
    left[64 : 64 + SEQ, :] = drive - drive_high
    right[...] = jnp.zeros((128, VECTOR), F32)
    right[:SEQ, :] = write_high
    right[32 : 32 + SEQ, :] = write - write_high
    right[64 : 64 + SEQ, :] = write_high
    for b in range(HIDDEN // 128):
        part = slice(b * 128, (b + 1) * 128)
        left_t[part, :] = left[:, part].T.astype(BF)
    left[:, :VECTOR] = jnp.zeros((128, VECTOR), F32)
    left[:SEQ, :VECTOR] = read
    for g in range(2):
        part = slice(g * 128, (g + 1) * 128)
        read_t[part, :] = left[:, part].T
    acc[...] = jnp.zeros((HIDDEN, 128), F32)

    stacked_row = iota((128, 128), 0) % 32
    lane = iota((128, 128), 1)

    for c in range(PAIRS):
        chunk(c).wait()
        for g in range(2):
            part = slice(g * 128, (g + 1) * 128)
            pair = [2 * c, 2 * c + 1]
            outer = project(
                left_t[g * 256 : (g + 1) * 256, :],
                jnp.concatenate(
                    [jnp.where(stacked_row == t, right[:, part], 0.0) for t in pair], axis=1
                ).astype(BF),
            )
            fresh = []
            for k in range(2):
                pieces = []
                for h in range(4):
                    rows = pl.ds(c * PAIR + k * HIDDEN + g * 256 + h * HEAD_DIM, HEAD_DIM)
                    keep = decays[2 * c + k, g * 4 + h : g * 4 + h + 1, :]
                    new = (
                        keep * state_ref[rows, :]
                        + outer[h * HEAD_DIM : (h + 1) * HEAD_DIM, k * 128 : (k + 1) * 128]
                    )
                    state_ref[rows, :] = new
                    pieces.append(new.astype(BF))
                fresh.append(jnp.concatenate(pieces, axis=0))
            reader = jnp.concatenate(
                [jnp.where(lane == t, read_t[part, :], 0.0) for t in pair], axis=0
            ).astype(BF)
            acc[g * 256 : (g + 1) * 256, :] += project(jnp.concatenate(fresh, axis=1), reader)
        chunk_out(c).start()

    for b in range(HIDDEN // 128):
        part = slice(b * 128, (b + 1) * 128)
        mixed_ref[:, part] = acc[part, :].T[:SEQ, :] + skip_wide[:, part] * value[:, part]

    for c in range(PAIRS):
        chunk_out(c).wait()


def mix(*operands):
    vmem = pl.BlockSpec(memory_space=pltpu.VMEM)
    hbm = pl.BlockSpec(memory_space=pltpu.HBM)
    dma = pltpu.SemaphoreType.DMA
    return pl.pallas_call(
        mix_kernel,
        out_shape=(
            jax.ShapeDtypeStruct((SEQ, WIDTH), BF),
            jax.ShapeDtypeStruct((SEQ, HIDDEN), F32),
            jax.ShapeDtypeStruct((SEQ * HIDDEN, 128), F32),
        ),
        in_specs=[hbm] * len(operands),
        out_specs=(vmem, vmem, hbm),
        scratch_shapes=[pltpu.VMEM(x.shape, x.dtype) for x in operands]
        + [
            pltpu.VMEM((128, HIDDEN), F32),
            pltpu.VMEM((HIDDEN, 128), BF),
            pltpu.VMEM((128, VECTOR), F32),
            pltpu.VMEM((VECTOR, 128), F32),
            pltpu.VMEM((PAD, HEADS, 128), F32),
            pltpu.VMEM((HIDDEN, 128), F32),
            dma((len(operands) - 1,)),
            dma((PAIRS,)),
            dma((PAIRS,)),
        ],
        compiler_params=pltpu.CompilerParams(vmem_limit_bytes=VMEM_ALL),
        name="mix",
    )(*operands)


def moe_kernel(*refs):
    sources, out_ref, held = refs[:13], refs[13], refs[14:27]
    (
        normed_ref,
        gate_proj,
        heads_ref,
        group_gain_ref,
        out_proj,
        hid_ref,
        gain_ref,
        group_ref,
        expert_ref,
        choice_ref,
        wg,
        wu,
        wd,
    ) = held
    (
        part_ref,
        part_in,
        resid,
        route,
        send,
        recv,
        recv_sib,
        comb,
        perm,
        perm_back,
        rows_own,
        rows_sib,
        act,
        y_own,
        y_out,
        y_in,
        back,
        ret,
        w_sem,
        p_send,
        p_recv,
        d_send,
        d_recv,
        f_send,
        f_recv,
        s_send,
        s_recv,
        r_send,
        r_recv,
    ) = refs[27:]
    me = lax.axis_index("ep")
    tp = lax.axis_index("tp")
    mx = lax.rem(me, SIDE)
    my = lax.rem(lax.div(me, SIDE), SIDE)
    mz = lax.div(me, SIDE * SIDE)
    xs = [lax.rem(mx + d, SIDE) for d in range(SIDE)]
    zs = [lax.rem(mz + d, SIDE) * (SIDE * SIDE) for d in range(SIDE)]

    def each_peer(r, sign, act):
        def line(dy, first):
            y = lax.rem(my + SIDE + sign * dy, SIDE) * SIDE
            for dx in range(first, SIDE):
                act(dy * SIDE + dx, zs[sign * r % SIDE] + y + xs[sign * dx % SIDE])

        if r == 0:
            line(0, 1)

        @pl.loop(1 if r == 0 else 0, SIDE)
        def _(dy):
            line(dy, 0)

    sibling = {"tp": 1 - tp}

    def block(r, j):
        return pl.ds(pl.multiple_of(r * PLANE + j * ROWS, TILES), ROWS)

    bar = pltpu.get_barrier_semaphore()
    pl.semaphore_signal(bar, inc=1, device_id=sibling)

    for r in ORDER:
        each_peer(
            r, 1, lambda j, peer: pl.semaphore_signal(bar, inc=1, device_id={"ep": peer})
        )

    loads = [
        pltpu.make_async_copy(sources[n], held[n], w_sem.at[n]) for n in range(len(held))
    ]
    for n in [9, 0, 1, 2, 3, 4, 5, 6, 7, 8, 10, 11, 12]:
        loads[n].start()

    for load in loads[:4]:
        load.wait()
    gate = project(normed_ref[...], gate_proj[...]).astype(BF).astype(F32)
    gated = heads_ref[...] * (gate * jax.nn.sigmoid(gate))
    mixer_cols = pl.ds(pl.multiple_of(tp * HIDDEN, HIDDEN), HIDDEN)
    group_gain = group_gain_ref[mixer_cols].astype(F32).reshape(1, HIDDEN)
    mixed = []
    for g in range(2):
        cols = slice(g * 256, (g + 1) * 256)
        part = gated[:, cols]
        spread_ = lax.rsqrt(jnp.mean(part * part, axis=1, keepdims=True) + EPSILON)
        mixed.append(part * spread_ * group_gain[:, cols])
    mixed = jnp.concatenate(mixed, axis=1).astype(BF)
    loads[4].wait()
    part_ref[...] = project(mixed, out_proj[...])

    pl.semaphore_wait(bar, PEERS)

    swap = pltpu.make_async_remote_copy(
        part_ref, part_in, p_send, p_recv, device_id=sibling
    )
    swap.start()
    for load in loads[5:10]:
        load.wait()
    resid[16:PAD, :] = jnp.zeros((PAD - 16, WIDTH), F32)
    diagonal = iota((PAD, SEQ), 0) == iota((PAD, SEQ), 1)
    earlier = iota((PAD, SEQ), 1) < iota((PAD, SEQ), 0)
    valid = iota((PAD, 1), 0) < SEQ
    lines = [choice_ref[k : k + 1, :].astype(F32) for k in range(SLOTS)]
    chosen = [jnp.sum(jnp.where(diagonal, line, 0.0), axis=1, keepdims=True) for line in lines]
    codes = []
    for k in range(SLOTS):
        same = jnp.zeros((PAD, SEQ), F32)
        for line in lines:
            same = same + jnp.where((line == chosen[k]) & earlier, 1.0, 0.0)
        rank = jnp.sum(same, axis=1, keepdims=True).astype(jnp.int32)
        number = chosen[k].astype(jnp.int32)
        x = (number % SIDE - mx + SIDE) % SIDE
        y = ((number // SIDE) % SIDE - my + SIDE) % SIDE
        z = (number // (SIDE * SIDE) - mz + SIDE) % SIDE
        slot = ((z * SIDE + y) * SIDE + x) * SLOTS + rank
        codes.append(jnp.where(valid, slot * TILES, -4096))
    lane = iota((PAD, SPREAD), 1)
    on_lane = lane % PAD == iota((PAD, SPREAD), 0)
    tile_of = iota((1, SPREAD), 1) // PAD
    code_rows = [
        jnp.sum(jnp.where(on_lane, code.astype(F32), 0.0), axis=0, keepdims=True).astype(jnp.int32)
        + tile_of
        for code in codes
    ]
    tile_down = iota((SPREAD, 1), 0) // PAD
    code_cols = [jnp.concatenate([code] * TILES, axis=0) + tile_down for code in codes]

    down_ = iota((128, 128), 0)
    over_ = iota((128, 128), 1)
    perm[...] = jnp.where(over_ == (down_ % 16) * TILES + down_ // 16, 1.0, 0.0).astype(BF)
    perm_back[...] = jnp.where(down_ == (over_ % 16) * TILES + over_ // 16, 1.0, 0.0).astype(BF)

    for r in range(SIDE):
        down = iota((PLANE, SPREAD), 0) + r * PLANE
        hit = (down == code_rows[0]) | (down == code_rows[1]) | (down == code_rows[2])
        route[r * PLANE : (r + 1) * PLANE, :] = jnp.where(hit, 1.0, 0.0).astype(BF)
    swap.wait_recv()
    resid[:SEQ, :] = hid_ref[...].astype(F32) + (part_ref[...] + part_in[...])
    total = resid[...]
    scale = lax.rsqrt(jnp.mean(total * total, axis=1, keepdims=True) + EPSILON)
    ffn_in = (total * scale * gain_ref[...].astype(F32).reshape(1, WIDTH)).astype(BF)

    @pl.when(tp == 0)
    def _():
        rows_own[:PAD, :] = ffn_in[:, :HALF]

    @pl.when(tp == 1)
    def _():
        rows_own[:PAD, :] = ffn_in[:, HALF:]

    mine = rows_own[:PAD, :].astype(F32)
    spread = jnp.concatenate(
        [mine[:, c * 128 : (c + 1) * 128] for c in range(TILES)], axis=0
    ).astype(BF)

    for r in ORDER:
        rows = project(route[r * PLANE : (r + 1) * PLANE, :], spread).astype(BF)
        send[r * PLANE : (r + 1) * PLANE, :] = rows
        if r == 0:
            recv[:ROWS, :] = rows[:ROWS, :]

        def dispatch(j, peer, r=r):
            pltpu.make_async_remote_copy(
                send.at[block(r, j)],
                recv.at[block(r, j)],
                d_send,
                d_recv.at[r],
                device_id={"ep": peer},
            ).start()

        each_peer(r, 1, dispatch)

    group_exp = jnp.exp(nt_dot(ffn_in, group_ref[...]))
    first = chosen[0].astype(jnp.int32) // GROUP_SIZE
    in_group = iota(group_exp.shape, 1) == first
    chosen_prob = jnp.sum(jnp.where(in_group, group_exp, 0.0), axis=1, keepdims=True) / jnp.sum(
        group_exp, axis=1, keepdims=True
    )
    logits = nt_dot(ffn_in, expert_ref[...])
    place = iota(logits.shape, 1)
    picked = [
        jnp.exp(
            jnp.sum(
                jnp.where(place == number.astype(jnp.int32), logits, 0.0), axis=1, keepdims=True
            )
        )
        for number in chosen
    ]
    below = picked[0] + picked[1] + picked[2]
    gates = [jnp.concatenate([chosen_prob * p / below] * TILES, axis=0) for p in picked]
    for r in range(SIDE):
        over = iota((SPREAD, PLANE), 1) + r * PLANE
        weights = jnp.where(over == code_cols[0], gates[0], 0.0)
        weights = jnp.where(over == code_cols[1], gates[1], weights)
        weights = jnp.where(over == code_cols[2], gates[2], weights)
        comb[:, r * PLANE : (r + 1) * PLANE] = weights.astype(BF)

    def relay(source, target, r):
        for b in range(3 * r, 3 * r + 3):
            moved = project(perm[...], source[b * 128 : (b + 1) * 128, :]).astype(BF)
            for c in range(TILES):
                target[b * 16 : (b + 1) * 16, c * 128 : (c + 1) * 128] = moved[
                    c * 16 : (c + 1) * 16, :
                ]

    def forward(r):
        whole = pl.ds(r * PLANE, PLANE)
        return pltpu.make_async_remote_copy(
            recv.at[whole], recv_sib.at[whole], f_send.at[r], f_recv.at[r], device_id=sibling
        )

    def landed(buffer, sem, r):
        low = ROWS if r == 0 else r * PLANE
        part = buffer.at[pl.ds(low, (r + 1) * PLANE - low)]
        return pltpu.make_async_copy(part, part, sem.at[r])

    own_rows = pl.ds(pl.multiple_of(tp * HALF, HALF), HALF)
    sib_rows = pl.ds(pl.multiple_of((1 - tp) * HALF, HALF), HALF)

    def arrive(r):
        landed(recv, d_recv, r).wait()
        forward(r).start()
        relay(recv, rows_own, r)

    def from_sibling(r):
        forward(r).wait_recv()
        relay(recv_sib, rows_sib, r)

    def hand(m):
        lines_ = pl.ds(m * BATCH, BATCH)
        return pltpu.make_async_remote_copy(
            y_out.at[lines_], y_in.at[lines_], s_send.at[m], s_recv.at[m], device_id=sibling
        )

    def expert(m):
        lines_ = slice(m * BATCH, (m + 1) * BATCH)
        for n in range(2):
            cols = slice(n * 256, (n + 1) * 256)
            gated = project(rows_own[lines_, :], wg[own_rows, cols]) + project(
                rows_sib[lines_, :], wg[sib_rows, cols]
            )
            upped = project(rows_own[lines_, :], wu[own_rows, cols]) + project(
                rows_sib[lines_, :], wu[sib_rows, cols]
            )
            act[lines_, cols] = (gated * jax.nn.sigmoid(gated) * upped).astype(BF)
        y_out[lines_, :] = project(act[lines_, :], wd[:, sib_rows]).astype(BF)
        hand(m).start()
        y_own[lines_, :] = project(act[lines_, :], wd[:, own_rows])

    def give_back(r):
        for b in range(3 * r, 3 * r + 3):
            lines_ = slice(b * 16, (b + 1) * 16)
            summed = (y_own[lines_, :] + y_in[lines_, :].astype(F32)).astype(BF)
            stacked = jnp.concatenate(
                [summed[:, c * 128 : (c + 1) * 128] for c in range(TILES)], axis=0
            )
            rows = project(perm_back[...], stacked).astype(BF)
            back[b * 128 : (b + 1) * 128, :] = rows
            if b == 0:
                ret[:ROWS, :] = rows[:ROWS, :]

        def send_back(j, peer):
            pltpu.make_async_remote_copy(
                back.at[block(r, j)],
                ret.at[block(r, j)],
                r_send,
                r_recv.at[r],
                device_id={"ep": peer},
            ).start()

        each_peer(r, -1, send_back)

    arrive(2)
    arrive(3)
    from_sibling(2)
    from_sibling(3)
    for load in loads[10:]:
        load.wait()
    expert(1)
    arrive(1)
    arrive(0)
    hand(1).wait_recv()
    give_back(2)
    give_back(3)
    from_sibling(1)
    from_sibling(0)
    expert(0)
    hand(0).wait_recv()
    give_back(1)
    give_back(0)
    merged = None
    for r in ORDER:
        landed(ret, r_recv, r).wait()
        cols = slice(r * PLANE, (r + 1) * PLANE)
        term = project(comb[:, cols], ret[cols, :])
        merged = term if merged is None else merged + term
    half = resid[:, own_rows]
    for c in range(TILES):
        cols = slice(c * 128, (c + 1) * 128)
        line = half[:, cols] + merged[c * PAD : (c + 1) * PAD, :]
        out_ref[:, cols] = line[:SEQ, :].astype(BF)

    swap.wait_send()
    for m in range(2):
        hand(m).wait_send()
    for r in range(SIDE):
        forward(r).wait_send()
    sent = send.at[pl.ds(ROWS, TOTAL - ROWS)]
    pltpu.make_async_copy(sent, sent, d_send).wait()
    gone = back.at[pl.ds(ROWS, TOTAL - ROWS)]
    pltpu.make_async_copy(gone, gone, r_send).wait()


def moe(*operands):
    vmem = pl.BlockSpec(memory_space=pltpu.VMEM)
    hbm = pl.BlockSpec(memory_space=pltpu.HBM)
    dma = pltpu.SemaphoreType.DMA
    slots = PEERS * SLOTS
    return pl.pallas_call(
        moe_kernel,
        out_shape=jax.ShapeDtypeStruct((SEQ, HALF), BF),
        in_specs=[hbm] * len(operands),
        out_specs=vmem,
        scratch_shapes=[pltpu.VMEM(x.shape, x.dtype) for x in operands]
        + [
            pltpu.VMEM((SEQ, WIDTH), F32),
            pltpu.VMEM((SEQ, WIDTH), F32),
            pltpu.VMEM((PAD, WIDTH), F32),
            pltpu.VMEM((TOTAL, SPREAD), BF),
            pltpu.VMEM((TOTAL, 128), BF),
            pltpu.VMEM((TOTAL, 128), BF),
            pltpu.VMEM((TOTAL, 128), BF),
            pltpu.VMEM((SPREAD, TOTAL), BF),
            pltpu.VMEM((128, 128), BF),
            pltpu.VMEM((128, 128), BF),
            pltpu.VMEM((slots, HALF), BF),
            pltpu.VMEM((slots, HALF), BF),
            pltpu.VMEM((slots, HIDDEN), BF),
            pltpu.VMEM((slots, HALF), F32),
            pltpu.VMEM((slots, HALF), BF),
            pltpu.VMEM((slots, HALF), BF),
            pltpu.VMEM((TOTAL, 128), BF),
            pltpu.VMEM((TOTAL, 128), BF),
            dma((len(operands),)),
            dma,
            dma,
            dma,
            dma((SIDE,)),
            dma((SIDE,)),
            dma((SIDE,)),
            dma((2,)),
            dma((2,)),
            dma,
            dma((SIDE,)),
        ],
        compiler_params=pltpu.CompilerParams(
            collective_id=0, has_side_effects=True, vmem_limit_bytes=VMEM_ALL
        ),
        name="moe",
    )(*operands)


def on_device(
    hidden,
    mixer_gain,
    gate_proj,
    value_proj,
    write_proj,
    read_proj,
    step_proj,
    step_bias,
    decay_log,
    skip_gain,
    value_taps,
    write_taps,
    read_taps,
    value_tail,
    write_tail,
    read_tail,
    scan_state,
    group_gain,
    out_proj,
    ffn_gain,
    group_router,
    expert_router,
    expert_choice,
    expert_gate,
    expert_up,
    expert_down,
):
    mixer_in, heads, new_state = mix(
        hidden,
        mixer_gain,
        step_proj.T,
        step_bias.reshape(1, -1),
        decay_log.reshape(1, -1),
        skip_gain.reshape(1, -1),
        value_proj,
        write_proj,
        read_proj,
        value_taps,
        write_taps,
        read_taps,
        value_tail.transpose(1, 0, 2),
        write_tail.transpose(1, 0, 2),
        read_tail.transpose(1, 0, 2),
        scan_state.reshape(SEQ * HIDDEN, 128),
    )
    layer_out = moe(
        mixer_in,
        gate_proj,
        heads,
        group_gain,
        out_proj,
        hidden,
        ffn_gain,
        group_router.T,
        expert_router.T,
        expert_choice.T,
        expert_gate[0],
        expert_up[0],
        expert_down[0],
    )
    return (layer_out, new_state.reshape(scan_state.shape))


def solution(mesh):
    placed = (
        P("ep", None),
        P(),
        P(None, "tp"),
        P(None, "tp"),
        P(None, "tp"),
        P(None, "tp"),
        P(),
        P(),
        P(),
        P(),
        P(),
        P(),
        P(),
        P("ep", None, "tp"),
        P("ep", None, "tp"),
        P("ep", None, "tp"),
        P("ep", "tp", None, None),
        P(),
        P("tp", None),
        P(),
        P(),
        P(),
        P("ep", None),
        P("ep", None, "tp"),
        P("ep", None, "tp"),
        P("ep", "tp", None),
    )
    return jax.shard_map(
        on_device,
        mesh=mesh,
        in_specs=placed,
        out_specs=(P("ep", "tp"), P("ep", "tp", None, None)),
        check_vma=False,
    )
```

```python
import jax
import jax.numpy as jnp
import numpy as np
from jax import lax
from jax.experimental import pallas as pl
from jax.experimental.pallas import tpu as pltpu
from jax.sharding import PartitionSpec as P

GROUP_SIZE = 8
EPSILON = 1e-06
SIDE = 4
PEERS = 64
SLOTS = 3
WIDTH = 2048
HALF = 1024
HIDDEN = 512
TILES = 8
ROWS = SLOTS * TILES
PLANE = 16 * ROWS
TOTAL = PEERS * ROWS
SEQ = 22
PAD = 24
SPREAD = TILES * PAD
HEADS = 8
HEAD_DIM = 64
VECTOR = 256
BF = jnp.bfloat16
F32 = jnp.float32
VMEM_LIMIT = 50 * 1024 * 1024
HOPS = (0, 1, 2, 1)
OFFSETS = sorted(
    ((z, y, x) for z in range(SIDE) for y in range(SIDE) for x in range(SIDE)),
    key=lambda o: (sum(HOPS[d] for d in o), o),
)
RANKS = np.zeros((1, PEERS), np.float32)
for _rank, (_z, _y, _x) in enumerate(OFFSETS):
    RANKS[0, (_z * SIDE + _y) * SIDE + _x] = _rank
PIECES = 4
SPANS = ((0, 4), (4, 10), (10, 16), (16, 22))
SMALL = ("hid", "gain", "step", "bias", "rate", "skip", "choice", "ranks")
TAPS = ("value_taps", "write_taps", "read_taps", "value_tail", "write_tail", "read_tail")
PROJECTIONS = ("value", "write", "read", "gate")
LATER = ("group_gain", "out", "ffn_gain", "group", "expert")
EXPERT = ("wg", "wu", "wd")
INPUTS = SMALL + PROJECTIONS + TAPS + LATER + EXPERT


def nt_dot(left, right):
    return lax.dot_general(left, right, (((1,), (1,)), ((), ())), preferred_element_type=F32)


def project(left, right):
    return jnp.dot(left, right, preferred_element_type=F32)


def iota(shape, dim):
    return lax.broadcasted_iota(jnp.int32, shape, dim)


def silu(x):
    return x * jax.nn.sigmoid(x)


def layer_kernel(*refs):
    count = len(INPUTS)
    sources, state_hbm = refs[:count], refs[count]
    out_ref, state_ref = refs[count + 1 : count + 3]
    held = dict(zip(INPUTS, refs[count + 3 : 2 * count + 3]))
    (
        left,
        left_t,
        right,
        read_t,
        decays,
        acc,
        part_out,
        part_in,
        resid,
        route,
        send,
        recv,
        gate_sum,
        up_sum,
        comb,
        perm,
        perm_back,
        rows_own,
        rows_sib,
        act,
        y_own,
        y_out,
        y_in,
        back,
        ret,
        load_sem,
        state_sem,
        p_send,
        p_recv,
        d_send,
        d_recv,
        f_send,
        f_recv,
        s_send,
        s_recv,
        r_send,
        r_recv,
    ) = refs[2 * count + 3 :]
    me = lax.axis_index("ep")
    tp = lax.axis_index("tp")
    mx = lax.rem(me, SIDE)
    my = lax.rem(lax.div(me, SIDE), SIDE)
    mz = lax.div(me, SIDE * SIDE)
    xs = [lax.rem(mx + d, SIDE) for d in range(SIDE)]
    ys = [lax.rem(my + d, SIDE) * SIDE for d in range(SIDE)]
    zs = [lax.rem(mz + d, SIDE) * (SIDE * SIDE) for d in range(SIDE)]
    sibling = {"tp": 1 - tp}

    def peer(i, sign):
        z, y, x = OFFSETS[i]
        return {"ep": zs[sign * z % SIDE] + ys[sign * y % SIDE] + xs[sign * x % SIDE]}

    loads = {
        name: pltpu.make_async_copy(sources[n], held[name], load_sem.at[n])
        for n, name in enumerate(INPUTS)
    }

    def start(*names):
        for name in names:
            loads[name].start()

    def wait(*names):
        for name in names:
            loads[name].wait()

    start(*SMALL, *TAPS, "value")

    bar = pltpu.get_barrier_semaphore()
    for i in range(PEERS - 1, 0, -1):
        pl.semaphore_signal(bar, inc=1, device_id=peer(i, 1))
    pl.semaphore_signal(bar, inc=1, device_id=sibling)
    start("write", "read")

    def span(n):
        low, high = SPANS[n]
        rows = pl.ds(low * HIDDEN, (high - low) * HIDDEN)
        return pltpu.make_async_copy(state_hbm.at[rows], state_ref.at[rows], state_sem.at[n])

    wait(*SMALL)
    start("gate")
    wide = held["hid"][...].astype(F32)
    scale = lax.rsqrt(jnp.mean(wide * wide, axis=1, keepdims=True) + EPSILON)
    mixer_in = (wide * scale * held["gain"][...].astype(F32).reshape(1, WIDTH)).astype(BF)

    def local_heads(line):
        return jnp.where(tp == 0, line[:, :HEADS], line[:, HEADS:])

    bias = local_heads(held["bias"][...])
    rate = jnp.exp(local_heads(held["rate"][...]))
    skip = local_heads(held["skip"][...])
    raw = local_heads(nt_dot(mixer_in, held["step"][...])) + bias
    step = jnp.maximum(raw, 0.0) + jnp.log1p(jnp.exp(-jnp.abs(raw)))
    decay = jnp.exp(-step * rate)
    for h in range(HEADS):
        decays[:SEQ, h, :] = jnp.broadcast_to(decay[:, h : h + 1], (SEQ, 128))
    span(0).start()
    span(1).start()

    wait("value", *TAPS)

    def convolve(name, newest, width):
        cols = pl.ds(pl.multiple_of(tp * width, width), width)
        taps = held[name + "_taps"][:, cols].astype(F32)
        summed = taps[3:4, :] * newest.astype(BF).astype(F32)
        for offset in range(3):
            summed = summed + taps[offset : offset + 1, :] * held[name + "_tail"][offset].astype(
                F32
            )
        return silu(summed)

    value = convolve("value", project(mixer_in, held["value"][...]), HIDDEN)
    span(2).start()
    span(3).start()
    wait("write", "read")
    start(*LATER)
    write = convolve("write", project(mixer_in, held["write"][...]), VECTOR)
    read = convolve("read", project(mixer_in, held["read"][...]), VECTOR)
    wait("gate")
    gate = silu(project(mixer_in, held["gate"][...]).astype(BF).astype(F32))

    head_of = iota((1, HIDDEN), 1) // HEAD_DIM
    step_wide = jnp.zeros((SEQ, HIDDEN), F32)
    decay_wide = jnp.zeros((SEQ, HIDDEN), F32)
    skip_wide = jnp.zeros((1, HIDDEN), F32)
    for h in range(HEADS):
        step_wide = jnp.where(head_of == h, step[:, h : h + 1], step_wide)
        decay_wide = jnp.where(head_of == h, decay[:, h : h + 1], decay_wide)
        skip_wide = jnp.where(head_of == h, skip[:, h : h + 1], skip_wide)
    drive = step_wide * value
    left[:, :VECTOR] = jnp.zeros((128, VECTOR), F32)
    left[:SEQ, :VECTOR] = read
    for g in range(2):
        part = slice(g * 128, (g + 1) * 128)
        read_t[part, :] = left[:, part].T
    acc[...] = jnp.zeros((HIDDEN, 128), F32)
    lane = iota((128, 128), 1)

    for n, (low, high) in enumerate(SPANS):
        span(n).wait()
        for g in range(2):
            part = slice(g * 128, (g + 1) * 128)
            block_ = slice(g * 256, (g + 1) * 256)
            stream = jnp.concatenate(
                [
                    state_ref[t * HIDDEN + g * 256 : t * HIDDEN + (g + 1) * 256, :].astype(BF)
                    for t in range(low, high)
                ],
                axis=1,
            )
            reader = jnp.concatenate(
                [jnp.where(lane == t, read_t[part, :], 0.0).astype(BF) for t in range(low, high)],
                axis=0,
            )
            acc[block_, :] += project(stream, reader)
    wait("group_gain")
    mixer_cols = pl.ds(pl.multiple_of(tp * HIDDEN, HIDDEN), HIDDEN)
    group_gain = held["group_gain"][mixer_cols].astype(F32).reshape(1, HIDDEN)
    mixed = []
    for g in range(2):
        part = slice(g * 128, (g + 1) * 128)
        cols = slice(g * 256, (g + 1) * 256)
        old = jnp.concatenate(
            [acc[g * 256 + b * 128 : g * 256 + (b + 1) * 128, :].T[:SEQ, :] for b in range(2)],
            axis=1,
        )
        overlap = jnp.sum(write[:, part] * read[:, part], axis=1, keepdims=True)
        heads = (
            decay_wide[:, cols] * old
            + overlap * drive[:, cols]
            + skip_wide[:, cols] * value[:, cols]
        )
        gated = heads * gate[:, cols]
        level = lax.rsqrt(jnp.mean(gated * gated, axis=1, keepdims=True) + EPSILON)
        mixed.append(gated * level * group_gain[:, cols])
    mixed = jnp.concatenate(mixed, axis=1).astype(BF)
    wait("out")
    pl.semaphore_wait(bar, PEERS)

    def swap(n):
        cols = pl.ds(n * HALF, HALF)
        return pltpu.make_async_remote_copy(
            part_out.at[:, cols], part_in.at[:, cols], p_send.at[n], p_recv.at[n], device_id=sibling
        )

    for n in range(2):
        cols = slice(n * HALF, (n + 1) * HALF)
        part_out[:, cols] = project(mixed, held["out"][:, cols])
        swap(n).start()
    start(*EXPERT)
    wait("ffn_gain", "group", "expert")
    resid[16:PAD, :] = jnp.zeros((PAD - 16, WIDTH), F32)
    diagonal = iota((PAD, SEQ), 0) == iota((PAD, SEQ), 1)
    earlier = iota((PAD, SEQ), 1) < iota((PAD, SEQ), 0)
    valid = iota((PAD, 1), 0) < SEQ
    lines = [held["choice"][k : k + 1, :].astype(F32) for k in range(SLOTS)]
    chosen = [jnp.sum(jnp.where(diagonal, line, 0.0), axis=1, keepdims=True) for line in lines]
    codes = []
    for k in range(SLOTS):
        same = jnp.zeros((PAD, SEQ), F32)
        for line in lines:
            same = same + jnp.where((line == chosen[k]) & earlier, 1.0, 0.0)
        rank = jnp.sum(same, axis=1, keepdims=True).astype(jnp.int32)
        number = chosen[k].astype(jnp.int32)
        x = (number % SIDE - mx + SIDE) % SIDE
        y = ((number // SIDE) % SIDE - my + SIDE) % SIDE
        z = (number // (SIDE * SIDE) - mz + SIDE) % SIDE
        seat = jnp.where(iota((PAD, PEERS), 1) == (z * SIDE + y) * SIDE + x, held["ranks"][...], 0.0)
        slot = jnp.sum(seat, axis=1, keepdims=True).astype(jnp.int32) * SLOTS + rank
        codes.append(jnp.where(valid, slot * TILES, -4096))
    lane = iota((PAD, SPREAD), 1)
    on_lane = lane % PAD == iota((PAD, SPREAD), 0)
    tile_of = iota((1, SPREAD), 1) // PAD
    code_rows = [
        jnp.sum(jnp.where(on_lane, code.astype(F32), 0.0), axis=0, keepdims=True).astype(jnp.int32)
        + tile_of
        for code in codes
    ]
    for r in range(SIDE):
        down = iota((PLANE, SPREAD), 0) + r * PLANE
        hit = (down == code_rows[0]) | (down == code_rows[1]) | (down == code_rows[2])
        route[r * PLANE : (r + 1) * PLANE, :] = jnp.where(hit, 1.0, 0.0).astype(BF)
    swap(0).wait_recv()
    swap(1).wait_recv()
    resid[:SEQ, :] = held["hid"][...].astype(F32) + (part_out[...] + part_in[...])
    total = resid[...]
    scale = lax.rsqrt(jnp.mean(total * total, axis=1, keepdims=True) + EPSILON)
    ffn_in = (total * scale * held["ffn_gain"][...].astype(F32).reshape(1, WIDTH)).astype(BF)

    @pl.when(tp == 0)
    def _():
        rows_own[:PAD, :] = ffn_in[:, :HALF]

    @pl.when(tp == 1)
    def _():
        rows_own[:PAD, :] = ffn_in[:, HALF:]

    mine = rows_own[:PAD, :].astype(F32)
    spread = jnp.concatenate(
        [mine[:, c * 128 : (c + 1) * 128] for c in range(TILES)], axis=0
    ).astype(BF)

    def block(i):
        return pl.ds(i * ROWS, ROWS)

    for r in reversed(range(SIDE)):
        rows = project(route[r * PLANE : (r + 1) * PLANE, :], spread).astype(BF)
        send[r * PLANE : (r + 1) * PLANE, :] = rows
        if r == 0:
            recv[:ROWS, :] = rows[:ROWS, :]
        for i in reversed(range(max(16 * r, 1), 16 * r + 16)):
            pltpu.make_async_remote_copy(
                send.at[block(i)], recv.at[block(i)], d_send, d_recv.at[r], device_id=peer(i, 1)
            ).start()

    tile_down = iota((SPREAD, 1), 0) // PAD
    code_cols = [jnp.concatenate([code] * TILES, axis=0) + tile_down for code in codes]

    down_ = iota((128, 128), 0)
    over_ = iota((128, 128), 1)
    perm[...] = jnp.where(over_ == (down_ % 16) * TILES + down_ // 16, 1.0, 0.0).astype(BF)
    perm_back[...] = jnp.where(down_ == (over_ % 16) * TILES + over_ // 16, 1.0, 0.0).astype(BF)
    drive_high = drive.astype(BF).astype(F32)
    write_high = write.astype(BF).astype(F32)
    left[...] = jnp.zeros((128, HIDDEN), F32)
    left[:SEQ, :] = drive_high
    left[32 : 32 + SEQ, :] = drive_high
    left[64 : 64 + SEQ, :] = drive - drive_high
    right[...] = jnp.zeros((128, VECTOR), F32)
    right[:SEQ, :] = write_high
    right[32 : 32 + SEQ, :] = write - write_high
    right[64 : 64 + SEQ, :] = write_high
    for b in range(HIDDEN // 128):
        part = slice(b * 128, (b + 1) * 128)
        left_t[part, :] = left[:, part].T.astype(BF)

    group_exp = jnp.exp(nt_dot(ffn_in, held["group"][...]))
    first = chosen[0].astype(jnp.int32) // GROUP_SIZE
    in_group = iota(group_exp.shape, 1) == first
    chosen_prob = jnp.sum(jnp.where(in_group, group_exp, 0.0), axis=1, keepdims=True) / jnp.sum(
        group_exp, axis=1, keepdims=True
    )
    logits = nt_dot(ffn_in, held["expert"][...])
    place = iota(logits.shape, 1)
    picked = [
        jnp.exp(
            jnp.sum(
                jnp.where(place == number.astype(jnp.int32), logits, 0.0), axis=1, keepdims=True
            )
        )
        for number in chosen
    ]
    below = picked[0] + picked[1] + picked[2]
    gates = [jnp.concatenate([chosen_prob * p / below] * TILES, axis=0) for p in picked]
    for r in range(SIDE):
        over = iota((SPREAD, PLANE), 1) + r * PLANE
        weights = jnp.where(over == code_cols[0], gates[0], 0.0)
        weights = jnp.where(over == code_cols[1], gates[1], weights)
        weights = jnp.where(over == code_cols[2], gates[2], weights)
        comb[:, r * PLANE : (r + 1) * PLANE] = weights.astype(BF)

    def tiles(n):
        return slice(n * 128, (n + 1) * 128)

    def relay(r):
        fresh = jnp.concatenate([recv[tiles(3 * r + k), :] for k in range(3)], axis=1)
        moved = project(perm[...], fresh).astype(BF)
        for k in range(3):
            b = 3 * r + k
            for c in range(TILES):
                rows_own[b * 16 : (b + 1) * 16, tiles(c)] = moved[c * 16 : (c + 1) * 16, tiles(k)]

    def forward(r):
        lines_ = pl.ds(r * 48, 48)
        return pltpu.make_async_remote_copy(
            rows_own.at[lines_], rows_sib.at[lines_], f_send.at[r], f_recv.at[r], device_id=sibling
        )

    def landed(buffer, sem, r):
        low = ROWS if r == 0 else r * PLANE
        part = buffer.at[pl.ds(low, (r + 1) * PLANE - low)]
        return pltpu.make_async_copy(part, part, sem.at[r])

    own_rows = pl.ds(pl.multiple_of(tp * HALF, HALF), HALF)
    sib_rows = pl.ds(pl.multiple_of((1 - tp) * HALF, HALF), HALF)

    def hand(r):
        lines_ = pl.ds(r * 48, 48)
        return pltpu.make_async_remote_copy(
            y_out.at[lines_], y_in.at[lines_], s_send.at[r], s_recv.at[r], device_id=sibling
        )

    def give_back(r):
        stacks = []
        for b in range(3 * r, 3 * r + 3):
            lines_ = slice(b * 16, (b + 1) * 16)
            summed = (y_own[lines_, :] + y_in[lines_, :].astype(F32)).astype(BF)
            stacks.append(jnp.concatenate([summed[:, tiles(c)] for c in range(TILES)], axis=0))
        rows = project(perm_back[...], jnp.concatenate(stacks, axis=1)).astype(BF)
        for k in range(3):
            back[tiles(3 * r + k), :] = rows[:, tiles(k)]
        if r == 0:
            ret[:ROWS, :] = rows[:ROWS, :128]
        for i in reversed(range(max(16 * r, 1), 16 * r + 16)):
            pltpu.make_async_remote_copy(
                back.at[block(i)], ret.at[block(i)], r_send, r_recv.at[r], device_id=peer(i, -1)
            ).start()

    for r in reversed(range(SIDE)):
        landed(recv, d_recv, r).wait()
        relay(r)
        forward(r).start()
    wait(*EXPERT)
    for n in range(2):
        cols = slice(n * 256, (n + 1) * 256)
        gate_sum[:, cols] = project(rows_own[...], held["wg"][own_rows, cols])
        up_sum[:, cols] = project(rows_own[...], held["wu"][own_rows, cols])
    for r in range(SIDE):
        forward(r).wait_recv()
    for n in range(2):
        cols = slice(n * 256, (n + 1) * 256)
        gated = gate_sum[:, cols] + project(rows_sib[...], held["wg"][sib_rows, cols])
        upped = up_sum[:, cols] + project(rows_sib[...], held["wu"][sib_rows, cols])
        act[:, cols] = (silu(gated) * upped).astype(BF)
    y_out[...] = project(act[...], held["wd"][:, sib_rows]).astype(BF)
    for r in reversed(range(SIDE)):
        hand(r).start()
    y_own[...] = project(act[...], held["wd"][:, own_rows])
    for r in reversed(range(SIDE)):
        hand(r).wait_recv()
        give_back(r)
    stacked_row = iota((128, 128), 0) % 32
    for c in range(SEQ // 2):
        pair = [2 * c, 2 * c + 1]
        for g in range(2):
            part = slice(g * 128, (g + 1) * 128)
            outer = project(
                left_t[g * 256 : (g + 1) * 256, :],
                jnp.concatenate(
                    [jnp.where(stacked_row == t, right[:, part], 0.0) for t in pair], axis=1
                ).astype(BF),
            )
            for k, t in enumerate(pair):
                for h in range(4):
                    rows = pl.ds(t * HIDDEN + g * 256 + h * HEAD_DIM, HEAD_DIM)
                    keep = decays[t, g * 4 + h : g * 4 + h + 1, :]
                    state_ref[rows, :] = (
                        keep * state_ref[rows, :]
                        + outer[h * HEAD_DIM : (h + 1) * HEAD_DIM, k * 128 : (k + 1) * 128]
                    )
    merged = None
    for r in range(SIDE):
        landed(ret, r_recv, r).wait()
        cols = slice(r * PLANE, (r + 1) * PLANE)
        term = project(comb[:, cols], ret[cols, :])
        merged = term if merged is None else merged + term
    half = resid[:, own_rows]
    for c in range(TILES):
        cols = slice(c * 128, (c + 1) * 128)
        line = half[:, cols] + merged[c * PAD : (c + 1) * PAD, :]
        out_ref[:, cols] = line[:SEQ, :].astype(BF)

    for n in range(2):
        swap(n).wait_send()
    for r in range(SIDE):
        hand(r).wait_send()
    for r in range(SIDE):
        forward(r).wait_send()
    sent = send.at[pl.ds(ROWS, TOTAL - ROWS)]
    pltpu.make_async_copy(sent, sent, d_send).wait()
    gone = back.at[pl.ds(ROWS, TOTAL - ROWS)]
    pltpu.make_async_copy(gone, gone, r_send).wait()


def layer(*operands):
    dma = pltpu.SemaphoreType.DMA
    slots = PEERS * SLOTS
    pinned = [pltpu.with_memory_space_constraint(x, pltpu.HBM) for x in operands]
    return pl.pallas_call(
        layer_kernel,
        out_shape=(pltpu.VMEM((SEQ, HALF), BF), pltpu.VMEM((SEQ * HIDDEN, 128), F32)),
        in_specs=[pl.BlockSpec(memory_space=pltpu.HBM)] * len(operands),
        out_specs=(pl.BlockSpec(memory_space=pltpu.VMEM),) * 2,
        scratch_shapes=[pltpu.VMEM(x.shape, x.dtype) for x in operands[:-1]]
        + [
            pltpu.VMEM((128, HIDDEN), F32),
            pltpu.VMEM((HIDDEN, 128), BF),
            pltpu.VMEM((128, VECTOR), F32),
            pltpu.VMEM((VECTOR, 128), F32),
            pltpu.VMEM((PAD, HEADS, 128), F32),
            pltpu.VMEM((HIDDEN, 128), F32),
            pltpu.VMEM((SEQ, WIDTH), F32),
            pltpu.VMEM((SEQ, WIDTH), F32),
            pltpu.VMEM((PAD, WIDTH), F32),
            pltpu.VMEM((TOTAL, SPREAD), BF),
            pltpu.VMEM((TOTAL, 128), BF),
            pltpu.VMEM((TOTAL, 128), BF),
            pltpu.VMEM((slots, HIDDEN), F32),
            pltpu.VMEM((slots, HIDDEN), F32),
            pltpu.VMEM((SPREAD, TOTAL), BF),
            pltpu.VMEM((128, 128), BF),
            pltpu.VMEM((128, 128), BF),
            pltpu.VMEM((slots, HALF), BF),
            pltpu.VMEM((slots, HALF), BF),
            pltpu.VMEM((slots, HIDDEN), BF),
            pltpu.VMEM((slots, HALF), F32),
            pltpu.VMEM((slots, HALF), BF),
            pltpu.VMEM((slots, HALF), BF),
            pltpu.VMEM((TOTAL, 128), BF),
            pltpu.VMEM((TOTAL, 128), BF),
            dma((len(INPUTS),)),
            dma((len(SPANS),)),
            dma((2,)),
            dma((2,)),
            dma,
            dma((SIDE,)),
            dma((SIDE,)),
            dma((SIDE,)),
            dma((SIDE,)),
            dma((SIDE,)),
            dma,
            dma((SIDE,)),
        ],
        compiler_params=pltpu.CompilerParams(
            collective_id=0, has_side_effects=True, vmem_limit_bytes=VMEM_LIMIT
        ),
        name="layer",
    )(*pinned)


def finish_kernel(rows_ref, state_ref, rows_out, state_out, sems):
    span = SEQ * HIDDEN // PIECES
    copies = [
        pltpu.make_async_copy(
            state_ref.at[pl.ds(n * span, span)], state_out.at[pl.ds(n * span, span)], sems.at[n]
        )
        for n in range(PIECES)
    ]
    copies.append(pltpu.make_async_copy(rows_ref, rows_out, sems.at[PIECES]))
    for copy in copies:
        copy.start()
    for copy in copies:
        copy.wait()


def finish(rows, state):
    hbm = pl.BlockSpec(memory_space=pltpu.HBM)
    vmem = pl.BlockSpec(memory_space=pltpu.VMEM)
    return pl.pallas_call(
        finish_kernel,
        out_shape=(
            jax.ShapeDtypeStruct(rows.shape, rows.dtype),
            jax.ShapeDtypeStruct(state.shape, state.dtype),
        ),
        in_specs=[vmem, vmem],
        out_specs=(hbm, hbm),
        scratch_shapes=[pltpu.SemaphoreType.DMA((PIECES + 1,))],
        compiler_params=pltpu.CompilerParams(vmem_limit_bytes=1024 * 1024),
        name="finish",
    )(*[pltpu.with_memory_space_constraint(x, pltpu.VMEM) for x in (rows, state)])


def on_device(
    hidden,
    mixer_gain,
    gate_proj,
    value_proj,
    write_proj,
    read_proj,
    step_proj,
    step_bias,
    decay_log,
    skip_gain,
    value_taps,
    write_taps,
    read_taps,
    value_tail,
    write_tail,
    read_tail,
    scan_state,
    group_gain,
    out_proj,
    ffn_gain,
    group_router,
    expert_router,
    expert_choice,
    expert_gate,
    expert_up,
    expert_down,
):
    layer_out, new_state = finish(*layer(
        hidden,
        mixer_gain,
        step_proj.T,
        step_bias.reshape(1, -1),
        decay_log.reshape(1, -1),
        skip_gain.reshape(1, -1),
        expert_choice.T,
        jnp.asarray(RANKS),
        value_proj,
        write_proj,
        read_proj,
        gate_proj,
        value_taps,
        write_taps,
        read_taps,
        value_tail.transpose(1, 0, 2),
        write_tail.transpose(1, 0, 2),
        read_tail.transpose(1, 0, 2),
        group_gain,
        out_proj,
        ffn_gain,
        group_router.T,
        expert_router.T,
        expert_gate[0],
        expert_up[0],
        expert_down[0],
        scan_state.reshape(SEQ * HIDDEN, 128),
    ))
    return (layer_out, new_state.reshape(scan_state.shape))


def solution(mesh):
    placed = (
        P("ep", None),
        P(),
        P(None, "tp"),
        P(None, "tp"),
        P(None, "tp"),
        P(None, "tp"),
        P(),
        P(),
        P(),
        P(),
        P(),
        P(),
        P(),
        P("ep", None, "tp"),
        P("ep", None, "tp"),
        P("ep", None, "tp"),
        P("ep", "tp", None, None),
        P(),
        P("tp", None),
        P(),
        P(),
        P(),
        P("ep", None),
        P("ep", None, "tp"),
        P("ep", None, "tp"),
        P("ep", "tp", None),
    )
    return jax.shard_map(
        on_device,
        mesh=mesh,
        in_specs=placed,
        out_specs=(P("ep", "tp"), P("ep", "tp", None, None)),
        check_vma=False,
    )
```
